32 devices in a mesh: sp: 8 (over z, y), tp: 4 (over x, core).
Axes of the slice: x: 2, y: 2, z: 4, core: 2. Of those that a mesh axis runs over, the one named last changes fastest.
Arguments:
- input_activations: bfloat16 [8192, 2048], P(('sp', 'tp')), may hold values from -6 to 6
- norm_gain: float32 [2048], replicated, may hold values from 0.5 to 1.5
- w_gate: bfloat16 [2048, 2048], P('sp', 'tp'), may hold values from -0.125 to 0.125
- w_value: bfloat16 [2048, 2048], P('sp', 'tp'), may hold values from -0.125 to 0.125
- w_state_in: bfloat16 [2048, 1024], P('sp', 'tp'), may hold values from -0.125 to 0.125
- w_state_out: bfloat16 [2048, 1024], P('sp', 'tp'), may hold values from -0.125 to 0.125
- w_step_forward: bfloat16 [2048, 32], P('sp', 'tp'), may hold values from -0.03125 to 0.03125
- w_step_backward: bfloat16 [2048, 32], P('sp', 'tp'), may hold values from -0.03125 to 0.03125
- step_offset: float32 [2, 32], P(None, 'tp'), may hold values from -0.5 to 0.5
- fading_speed: float32 [2, 32], P(None, 'tp'), may hold values from 0.3 to 1
- conv_value: float32 [3, 2048], P(None, 'tp'), may hold values from -3.5 to 3.5
- conv_state_in: float32 [3, 1024], P(None, 'tp'), may hold values from -3.5 to 3.5
- conv_state_out: float32 [3, 1024], P(None, 'tp'), may hold values from -3.5 to 3.5
- out_gain: float32 [2048], P('tp'), may hold values from 0.5 to 1.5
- w_out: bfloat16 [2048, 2048], P('tp', 'sp'), may hold values from -0.125 to 0.125
Outputs:
- mixer_out: bfloat16 [8192, 2048], P(('sp', 'tp'))
The draws below stay inside these ranges and needn't reach their ends.
All inputs are finite; a program needn't handle non-finite values.
Results may differ from the reference program's by a relative error of at most 0.015.
Values may be sent and summed in bfloat16 or wider, within the bound.
A program may use at most 128 MiB of HBM per device.

```python
import math
import jax
import jax.numpy as jnp
from jax import lax

D = 2048
HEADS = 32
HEAD_DIM = 64
GROUPS = 8
STATE = 128
BLOCK = 128
WIDTH = 2048
SEQ = 8192


def block_levels(rng, dims, split, low, high):
    gain, own = 1.0, jax.random.fold_in(rng, 6)
    for axis_at, shards_of in split:
        heights = jnp.exp(jax.random.uniform(jax.random.fold_in(own, axis_at), (shards_of,), jnp.float32, low / len(split), high / len(split)))
        gain = gain * jnp.repeat(heights, dims[axis_at] // shards_of).reshape([-1 if axis == axis_at else 1 for axis in range(len(dims))])
    return gain


def gaussian(rng, extent, spread, bound, shards=(), dtype=jnp.bfloat16):
    drawn = jax.random.normal(rng, extent, jnp.float32) * spread
    if len(shards) > 0:
        drawn = block_levels(rng, extent, shards, -0.22, 0.18) * drawn
    return jnp.clip(drawn, min=-bound, max=bound).astype(dtype)


def setup_inputs(seed: int = 0) -> dict:
    key_list = jax.random.split(jax.random.key(seed), 16)
    return {
        "input_activations": gaussian(key_list[0], (SEQ, D), 1.0, 6.0, ((0, 32),)),
        "norm_gain": jnp.clip(1.0 + 0.1 * jax.random.normal(key_list[1], (D,), jnp.float32), 0.5, 1.5),
        "w_gate": gaussian(key_list[2], (D, WIDTH), D ** -0.5, 0.125, ((0, 8), (1, 4))),
        "w_value": gaussian(key_list[3], (D, WIDTH), D ** -0.5, 0.125, ((0, 8), (1, 4))),
        "w_state_in": gaussian(key_list[4], (D, GROUPS * STATE), D ** -0.5, 0.125, ((0, 8), (1, 4))),
        "w_state_out": gaussian(key_list[5], (D, GROUPS * STATE), D ** -0.5, 0.125, ((0, 8), (1, 4))),
        "w_step_forward": gaussian(key_list[6], (D, HEADS), (16 * D) ** -0.5, 0.03125, ((0, 8), (1, 4))),
        "w_step_backward": gaussian(key_list[7], (D, HEADS), (16 * D) ** -0.5, 0.03125, ((0, 8), (1, 4))),
        "step_offset": jnp.clip(jax.random.uniform(key_list[8], (2, HEADS), jnp.float32, -0.5, 0.5) * block_levels(key_list[8], (2, HEADS), ((1, 4),), -0.4, 0.0), -0.5, 0.5),
        "fading_speed": jnp.clip(jnp.exp(math.log(1.0) - 1.2039728 * jax.random.uniform(key_list[9], (2, HEADS), jnp.float32) ** block_levels(key_list[9], (2, HEADS), ((1, 4),), -0.2, 0.2)), 0.3, 1.0),
        "conv_value": gaussian(key_list[10], (3, WIDTH), 3 ** -0.5, 3.5, ((1, 4),), jnp.float32),
        "conv_state_in": gaussian(key_list[11], (3, GROUPS * STATE), 3 ** -0.5, 3.5, ((1, 4),), jnp.float32),
        "conv_state_out": gaussian(key_list[12], (3, GROUPS * STATE), 3 ** -0.5, 3.5, ((1, 4),), jnp.float32),
        "out_gain": jnp.clip(1.0 + 0.1 * jax.random.normal(key_list[13], (WIDTH,), jnp.float32), 0.5, 1.5),
        "w_out": gaussian(key_list[14], (WIDTH, D), WIDTH ** -0.5, 0.125, ((0, 4), (1, 8))),
    }


epsilon = 1e-06
HIGHEST_PRECISION = lax.Precision.HIGHEST

def rms_rows(values):
    wide = values.astype(jnp.float32)
    return wide * lax.rsqrt(lax.optimization_barrier(jnp.mean(wide * wide, axis=-1, keepdims=True)) + epsilon)

def short_filter(values, taps):
    wide = values.astype(jnp.float32)
    padded = jnp.pad(wide, ((1, 1), (0, 0)))
    mixed = taps[0] * padded[:-2] + taps[1] * padded[1:-1] + taps[2] * padded[2:]
    return jax.nn.silu(mixed).astype(jnp.bfloat16)

def sweep(signal, step_size, rate, inward, outward):
    sequence_extent = signal.shape[0]
    count = sequence_extent // BLOCK
    ratio = HEADS // GROUPS
    blocks = signal.reshape(count, BLOCK, GROUPS, ratio, HEAD_DIM).astype(jnp.float32)
    step_blocks = step_size.reshape(count, BLOCK, GROUPS, ratio)
    inward_blocks = inward.reshape(count, BLOCK, GROUPS, STATE).astype(jnp.float32)
    outward_blocks = outward.reshape(count, BLOCK, GROUPS, STATE).astype(jnp.float32)
    log_decay = -step_blocks * rate.reshape(GROUPS, ratio)
    lower = (jnp.arange(BLOCK)[:, None] >= jnp.arange(BLOCK)[None, :])[:, :, None, None]

    def advance(state, inputs):
        values, steps, inner, outer, logs = inputs
        within = jnp.cumsum(logs, axis=0)
        gaps = within[:, None] - within[None]
        decay = jnp.where(lower, jnp.exp(jnp.where(lower, gaps, 0.0)), 0.0)
        intersect = jnp.einsum('qgn,kgn->qkg', outer, inner, precision=HIGHEST_PRECISION)
        weights_mix = intersect[..., None] * decay * steps[None]
        result = jnp.einsum('qkgr,kgrp->qgrp', weights_mix, values, precision=HIGHEST_PRECISION)
        result = result + jnp.einsum('qgn,grpn->qgrp', outer, state, precision=HIGHEST_PRECISION) * jnp.exp(within)[..., None]
        final = within[-1]
        scaling_factor = jnp.exp(final[None] - within) * steps
        added = jnp.einsum('qgn,qgrp->grpn', inner, values * scaling_factor[..., None], precision=HIGHEST_PRECISION)
        return (state * jnp.exp(final)[..., None, None] + added, result)
    start_state = jnp.zeros((GROUPS, ratio, HEAD_DIM, STATE), jnp.float32)
    _, outputs = lax.scan(advance, start_state, (blocks, step_blocks, inward_blocks, outward_blocks, log_decay))
    return outputs.reshape(sequence_extent, WIDTH)

def reference(input_activations, norm_gain, w_gate, w_value, w_state_in, w_state_out, w_step_forward, w_step_backward, step_offset, fading_speed, conv_value, conv_state_in, conv_state_out, out_gain, w_out):
    normed = (rms_rows(input_activations) * norm_gain).astype(jnp.bfloat16)

    def project(scaling_factor):
        return jnp.dot(normed, scaling_factor, preferred_element_type=jnp.float32).astype(jnp.bfloat16)
    gate = project(w_gate)
    value = project(w_value)
    inward_raw = project(w_state_in)
    outward_raw = project(w_state_out)
    raw_forward = project(w_step_forward)
    raw_backward = project(w_step_backward)
    shift = math.log(SEQ)
    step_forward = jax.nn.softplus(raw_forward.astype(jnp.float32) + step_offset[0] - shift)
    step_backward = jax.nn.softplus(raw_backward.astype(jnp.float32) + step_offset[1] - shift)
    signal = short_filter(value, conv_value).reshape(SEQ, HEADS, HEAD_DIM)
    inward = short_filter(inward_raw, conv_state_in).reshape(SEQ, GROUPS, STATE)
    outward = short_filter(outward_raw, conv_state_out).reshape(SEQ, GROUPS, STATE)
    forward = sweep(signal, step_forward, fading_speed[0], inward, outward)
    backward = sweep(signal[::-1], step_backward[::-1], fading_speed[1], inward[::-1], outward[::-1])[::-1]
    gated = (forward + backward) * jax.nn.silu(gate.astype(jnp.float32))
    grouped = rms_rows(gated.reshape(SEQ, GROUPS, WIDTH // GROUPS)).reshape(SEQ, WIDTH)
    mixed = (grouped * out_gain).astype(jnp.bfloat16)
    return jnp.dot(mixed, w_out, preferred_element_type=jnp.float32).astype(jnp.bfloat16)
```

```python
import functools
import math

import jax
import jax.numpy as jnp
from jax import lax
from jax.experimental import pallas as pl
from jax.experimental.pallas import tpu as pltpu
from jax.sharding import PartitionSpec as P

HEAD_DIM = 64
STATE = 128
BLOCK = 128
LANES = 128
EPSILON = 1e-06
HIGHEST = lax.Precision.HIGHEST
VMEM_LIMIT = 60 * 1024 * 1024


def rms_rows(values):
    wide = values.astype(jnp.float32)
    return wide * lax.rsqrt(jnp.mean(wide * wide, axis=-1, keepdims=True) + EPSILON)


def sigmoid(values):
    return 1.0 / (1.0 + jnp.exp(-values))


def softplus(values):
    return jnp.maximum(values, 0.0) + jnp.log1p(jnp.exp(-jnp.abs(values)))


def spread(columns, first, count):
    rows = columns.shape[0]
    lane = lax.broadcasted_iota(jnp.int32, (rows, LANES), 1)
    tiles = []
    for at in range(first, first + count, 2):
        low = jnp.broadcast_to(columns[:, at : at + 1], (rows, LANES))
        high = jnp.broadcast_to(columns[:, at + 1 : at + 2], (rows, LANES))
        tiles.append(jnp.where(lane < HEAD_DIM, low, high))
    return jnp.concatenate(tiles, axis=1)


def states_kernel(
    shape,
    proj_ref,
    edges_ref,
    taps_ref,
    offset_ref,
    rate_ref,
    signal_ref,
    inward_ref,
    outward_ref,
    within_ref,
    rows_ref,
    block_states_ref,
    block_logs_ref,
    sent_ref,
    padded,
    logs_total,
):
    groups, ratio, content, state_width, heads, shift = shape
    extent = proj_ref.shape[0]
    count = extent // BLOCK
    channels = content + 2 * state_width
    span = ratio * HEAD_DIM
    edge = edges_ref[...].astype(jnp.float32)
    padded[pl.ds(0, 8), :] = jnp.broadcast_to(edge[0:1], (8, channels))
    padded[pl.ds(extent + 8, 8), :] = jnp.broadcast_to(edge[1:2], (8, channels))

    def widen(at, _):
        start = pl.multiple_of(at * BLOCK, BLOCK)
        padded[pl.ds(pl.multiple_of(start + 8, 8), BLOCK), :] = proj_ref[
            pl.ds(start, BLOCK), content : content + channels
        ].astype(jnp.float32)
        return 0

    lax.fori_loop(0, count, widen, 0)
    row = lax.broadcasted_iota(jnp.int32, (BLOCK, BLOCK), 0)
    column = lax.broadcasted_iota(jnp.int32, (BLOCK, BLOCK), 1)
    lower = (row >= column).astype(jnp.float32)
    upper = (row <= column).astype(jnp.float32)
    lane = lax.broadcasted_iota(jnp.int32, (1, LANES), 1)

    def block(at, _):
        start = pl.multiple_of(at * BLOCK, BLOCK)
        here = pl.ds(start, BLOCK)
        filtered = []
        for first in range(0, channels, 2 * LANES):
            part = padded[pl.ds(start, BLOCK + 16), first : first + 2 * LANES]
            taps = taps_ref[:, first : first + 2 * LANES]
            mixed = (
                taps[0:1] * part[7 : 7 + BLOCK]
                + taps[1:2] * part[8 : 8 + BLOCK]
                + taps[2:3] * part[9 : 9 + BLOCK]
            )
            filtered.append((mixed * sigmoid(mixed)).astype(jnp.bfloat16))
        filtered = jnp.concatenate(filtered, axis=1)
        signal = filtered[:, :content]
        inward = filtered[:, content : content + state_width]
        signal_ref[here, :] = signal
        inward_ref[here, :] = inward
        outward_ref[here, :] = filtered[:, content + state_width :]
        raw = proj_ref[here, content + channels :].astype(jnp.float32)
        steps = softplus(raw + offset_ref[...] - shift)
        logs = -steps * rate_ref[...]
        ahead = jnp.dot(lower, logs, precision=HIGHEST, preferred_element_type=jnp.float32)
        behind = jnp.dot(upper, logs, precision=HIGHEST, preferred_element_type=jnp.float32)
        within = jnp.where(lane < heads, ahead, behind)
        final = jnp.where(lane < heads, within[BLOCK - 1 : BLOCK], within[0:1])
        within_ref[here, :] = within
        rows_ref[0 : 2 * heads, here] = within.T[0 : 2 * heads]
        rows_ref[2 * heads : 4 * heads, here] = steps.T[0 : 2 * heads]
        scale = jnp.exp(final - within) * steps
        for group in range(groups):
            wide = signal[:, group * span : (group + 1) * span].astype(jnp.float32)
            scaled = jnp.concatenate(
                [wide * spread(scale, way * heads + group * ratio, ratio) for way in range(2)],
                axis=1,
            ).astype(jnp.bfloat16)
            added = lax.dot_general(
                inward[:, group * STATE : (group + 1) * STATE],
                scaled,
                (((0,), (0,)), ((), ())),
                preferred_element_type=jnp.float32,
            )
            block_states_ref[group, at] = added
            block_logs_ref[group, at] = jnp.concatenate(
                [spread(final, way * heads + group * ratio, ratio) for way in range(2)], axis=1
            )
        return 0

    lax.fori_loop(0, count, block, 0)
    logs_total[...] = jnp.zeros_like(logs_total)
    for group in range(groups):

        def onward(at, state):
            return state * jnp.exp(block_logs_ref[group, at][:, :span]) + block_states_ref[
                group, at
            ][:, :span]

        def back(at, state):
            at = count - 1 - at
            return state * jnp.exp(block_logs_ref[group, at][:, span:]) + block_states_ref[
                group, at
            ][:, span:]

        def total(at, carried):
            return carried + block_logs_ref[group, at]

        empty = jnp.zeros((STATE, span), jnp.float32)
        here = slice(group * STATE, (group + 1) * STATE)
        sent_ref[here, :span] = lax.fori_loop(0, count, onward, empty).astype(jnp.bfloat16)
        sent_ref[here, span:] = lax.fori_loop(0, count, back, empty).astype(jnp.bfloat16)
        decayed = lax.fori_loop(0, count, total, jnp.zeros((1, 2 * span), jnp.float32))
        coarse = decayed.astype(jnp.bfloat16).astype(jnp.float32)
        logs_total[2 * group : 2 * group + 1, :] = coarse
        logs_total[2 * group + 1 : 2 * group + 2, :] = decayed - coarse
    sent_ref[groups * STATE :, :] = logs_total[...].astype(jnp.bfloat16)


def diagonal_kernel(shape, signal_ref, inward_ref, outward_ref, within_ref, rows_ref, result_ref):
    groups, ratio, heads = shape
    count = signal_ref.shape[0] // BLOCK
    row = lax.broadcasted_iota(jnp.int32, (BLOCK, BLOCK), 0)
    column = lax.broadcasted_iota(jnp.int32, (BLOCK, BLOCK), 1)
    lane = lax.broadcasted_iota(jnp.int32, (BLOCK, LANES), 1)

    def block(at, _):
        here = pl.ds(pl.multiple_of(at * BLOCK, BLOCK), BLOCK)
        within = within_ref[here, :]
        for group in range(groups):
            intersect = lax.dot_general(
                outward_ref[here, group * STATE : (group + 1) * STATE],
                inward_ref[here, group * STATE : (group + 1) * STATE],
                (((1,), (1,)), ((), ())),
                preferred_element_type=jnp.float32,
            )
            products = []
            for head in range(group * ratio, (group + 1) * ratio):
                other = heads + head
                gap_ahead = within[:, head : head + 1] - rows_ref[head : head + 1, here]
                gap_behind = within[:, other : other + 1] - rows_ref[other : other + 1, here]
                step_ahead = rows_ref[2 * heads + head : 2 * heads + head + 1, here]
                step_behind = rows_ref[2 * heads + other : 2 * heads + other + 1, here]
                gap = jnp.where(row >= column, gap_ahead, gap_behind)
                step = jnp.where(
                    row > column,
                    step_ahead,
                    jnp.where(row < column, step_behind, step_ahead + step_behind),
                )
                weights = (intersect * jnp.exp(gap) * step).astype(jnp.bfloat16)
                tile = head // 2 * 2 * HEAD_DIM
                products.append(
                    jnp.dot(
                        weights,
                        signal_ref[here, tile : tile + LANES],
                        preferred_element_type=jnp.float32,
                    )
                )
            for pair in range(ratio // 2):
                at_tile = (group * ratio + 2 * pair) * HEAD_DIM
                result_ref[here, at_tile : at_tile + LANES] = jnp.where(
                    lane < HEAD_DIM, products[2 * pair], products[2 * pair + 1]
                )
        return 0

    lax.fori_loop(0, count, block, 0)


def finish_kernel(
    shape,
    gathered_ref,
    block_states_ref,
    block_logs_ref,
    outward_ref,
    within_ref,
    diagonal_ref,
    proj_ref,
    gain_ref,
    mixed_ref,
    total,
):
    groups, ratio, heads = shape
    stretches = gathered_ref.shape[0]
    count = outward_ref.shape[0] // BLOCK
    span = ratio * HEAD_DIM
    me = lax.axis_index("sp")
    for group in range(groups):
        states = slice(group * STATE, (group + 1) * STATE)
        log_at = groups * STATE

        def incoming(source, state, lanes):
            logs = gathered_ref[source, log_at : log_at + 16, lanes].astype(jnp.float32)
            logs = logs[2 * group : 2 * group + 1] + logs[2 * group + 1 : 2 * group + 2]
            return state * jnp.exp(logs) + gathered_ref[source, states, lanes].astype(jnp.float32)

        empty = jnp.zeros((STATE, span), jnp.float32)
        ahead = lax.fori_loop(
            0, me, lambda hop, state: incoming(hop, state, slice(0, span)), empty
        )
        behind = lax.fori_loop(
            0,
            stretches - 1 - me,
            lambda hop, state: incoming(stretches - 1 - hop, state, slice(span, 2 * span)),
            empty,
        )
        wide = slice(group * span, (group + 1) * span)

        def back(hop, state):
            at = count - 1 - hop
            here = pl.ds(pl.multiple_of(at * BLOCK, BLOCK), BLOCK)
            carried = jnp.dot(
                outward_ref[here, states],
                state.astype(jnp.bfloat16),
                preferred_element_type=jnp.float32,
            )
            decay = spread(jnp.exp(within_ref[here, :]), heads + group * ratio, ratio)
            total[here, wide] = diagonal_ref[here, wide] + carried * decay
            return (
                state * jnp.exp(block_logs_ref[group, at][:, span:])
                + block_states_ref[group, at][:, span:]
            )

        lax.fori_loop(0, count, back, behind)

        def onward(at, state):
            here = pl.ds(pl.multiple_of(at * BLOCK, BLOCK), BLOCK)
            carried = jnp.dot(
                outward_ref[here, states],
                state.astype(jnp.bfloat16),
                preferred_element_type=jnp.float32,
            )
            decay = spread(jnp.exp(within_ref[here, :]), group * ratio, ratio)
            gate = proj_ref[here, wide].astype(jnp.float32)
            gated = (total[here, wide] + carried * decay) * (gate * sigmoid(gate))
            scale = lax.rsqrt(jnp.mean(gated * gated, axis=-1, keepdims=True) + EPSILON)
            mixed_ref[here, wide] = (gated * scale * gain_ref[:, wide]).astype(jnp.bfloat16)
            return (
                state * jnp.exp(block_logs_ref[group, at][:, :span])
                + block_states_ref[group, at][:, :span]
            )

        lax.fori_loop(0, count, onward, ahead)


def kernel_call(body, out_shape, scratch, micros):
    return pl.pallas_call(
        body,
        out_shape=out_shape,
        scratch_shapes=scratch,
        cost_estimate=pl.CostEstimate(
            flops=int(micros * 5e8), bytes_accessed=1 << 20, transcendentals=0
        ),
        compiler_params=pltpu.CompilerParams(vmem_limit_bytes=VMEM_LIMIT),
    )


def on_device(
    input_activations,
    norm_gain,
    w_gate,
    w_value,
    w_state_in,
    w_state_out,
    w_step_forward,
    w_step_backward,
    step_offset,
    fading_speed,
    conv_value,
    conv_state_in,
    conv_state_out,
    out_gain,
    w_out,
):
    stretches = lax.axis_size("sp")
    content = w_value.shape[1]
    state_width = w_state_in.shape[1]
    heads = w_step_forward.shape[1]
    groups = state_width // STATE
    ratio = heads // groups
    span = ratio * HEAD_DIM
    channels = content + 2 * state_width
    depth = w_gate.shape[0]
    spare = -2 * heads % LANES

    weights = jnp.concatenate(
        [
            w_gate,
            w_value,
            w_state_in,
            w_state_out,
            w_step_forward,
            w_step_backward,
            jnp.zeros((depth, spare), w_gate.dtype),
        ],
        axis=1,
    )
    all_weights = lax.all_gather(weights, "sp", axis=0, tiled=True)
    normed = (rms_rows(input_activations) * norm_gain).astype(jnp.bfloat16)
    tokens = lax.all_gather(normed, "tp", axis=0, tiled=True)
    proj = jnp.dot(tokens, all_weights, preferred_element_type=jnp.float32).astype(jnp.bfloat16)
    extent = tokens.shape[0]
    count = extent // BLOCK

    onward = [(i, i + 1) for i in range(stretches - 1)]
    back = [(target, source) for source, target in onward]
    low = lax.ppermute(proj[extent - 1 :, content : content + channels], "sp", onward)
    high = lax.ppermute(proj[:1, content : content + channels], "sp", back)
    edges = jnp.concatenate([low, high], axis=0)

    taps = jnp.concatenate([conv_value, conv_state_in, conv_state_out], axis=1)
    padding = ((0, 0), (0, spare))
    offset = jnp.pad(step_offset.reshape(1, 2 * heads), padding)
    rate = jnp.pad(fading_speed.reshape(1, 2 * heads), padding)
    shift = math.log(extent * stretches)

    bf16, f32 = jnp.bfloat16, jnp.float32
    made = jax.ShapeDtypeStruct
    sent_rows = groups * STATE + 16
    signal, inward, outward, within, rows, block_states, block_logs, sent = kernel_call(
        functools.partial(states_kernel, (groups, ratio, content, state_width, heads, shift)),
        (
            made((extent, content), bf16),
            made((extent, state_width), bf16),
            made((extent, state_width), bf16),
            made((extent, LANES), f32),
            made((4 * heads, extent), f32),
            made((groups, count, STATE, 2 * span), f32),
            made((groups, count, 1, 2 * span), f32),
            made((sent_rows, 2 * span), bf16),
        ),
        [pltpu.VMEM((extent + 16, channels), f32), pltpu.VMEM((16, 2 * span), f32)],
        15,
    )(proj, edges, taps, offset, rate)
    gathered = lax.all_gather(sent, "sp")
    diagonal = kernel_call(
        functools.partial(diagonal_kernel, (groups, ratio, heads)),
        made((extent, content), f32),
        [],
        15,
    )(signal, inward, outward, within, rows)
    mixed = kernel_call(
        functools.partial(finish_kernel, (groups, ratio, heads)),
        made((extent, content), bf16),
        [pltpu.VMEM((extent, content), f32)],
        15,
    )(
        gathered,
        block_states,
        block_logs,
        outward,
        within,
        diagonal,
        proj,
        out_gain.reshape(1, content),
    )
    full_out = lax.all_gather(w_out, "sp", axis=1, tiled=True)
    partial = jnp.dot(mixed, full_out, preferred_element_type=jnp.float32).astype(jnp.bfloat16)
    return lax.psum_scatter(partial, "tp", scatter_dimension=0, tiled=True)


def solution(mesh):
    return jax.shard_map(
        on_device,
        mesh=mesh,
        in_specs=(
            P(("sp", "tp"), None),
            P(),
            P("sp", "tp"),
            P("sp", "tp"),
            P("sp", "tp"),
            P("sp", "tp"),
            P("sp", "tp"),
            P("sp", "tp"),
            P(None, "tp"),
            P(None, "tp"),
            P(None, "tp"),
            P(None, "tp"),
            P(None, "tp"),
            P("tp"),
            P("tp", "sp"),
        ),
        out_specs=P(("sp", "tp"), None),
        check_vma=False,
    )
```

```python
import functools
import math

import jax
import jax.numpy as jnp
from jax import lax
from jax.experimental import pallas as pl
from jax.experimental.pallas import tpu as pltpu
from jax.sharding import PartitionSpec as P

HEAD_DIM = 64
STATE = 128
BLOCK = 128
LANES = 128
EPSILON = 1e-06
HIGHEST = lax.Precision.HIGHEST
VMEM_LIMIT = 60 * 1024 * 1024


def rms_rows(values):
    wide = values.astype(jnp.float32)
    return wide * lax.rsqrt(jnp.mean(wide * wide, axis=-1, keepdims=True) + EPSILON)


def sigmoid(values):
    return 1.0 / (1.0 + jnp.exp(-values))


def softplus(values):
    return jnp.maximum(values, 0.0) + jnp.log1p(jnp.exp(-jnp.abs(values)))


def spread(columns, first, count):
    rows = columns.shape[0]
    lane = lax.broadcasted_iota(jnp.int32, (rows, LANES), 1)
    tiles = []
    for at in range(first, first + count, 2):
        low = jnp.broadcast_to(columns[:, at : at + 1], (rows, LANES))
        high = jnp.broadcast_to(columns[:, at + 1 : at + 2], (rows, LANES))
        tiles.append(jnp.where(lane < HEAD_DIM, low, high))
    return jnp.concatenate(tiles, axis=1)


def states_kernel(
    shape,
    proj_ref,
    edges_ref,
    taps_ref,
    offset_ref,
    rate_ref,
    signal_ref,
    inward_ref,
    outward_ref,
    within_ref,
    rows_ref,
    block_states_ref,
    block_logs_ref,
    sent_ref,
    padded,
    logs_total,
):
    groups, ratio, content, state_width, heads, shift = shape
    extent = proj_ref.shape[0]
    count = extent // BLOCK
    channels = content + 2 * state_width
    span = ratio * HEAD_DIM
    edge = edges_ref[...].astype(jnp.float32)
    padded[pl.ds(0, 8), :] = jnp.broadcast_to(edge[0:1], (8, channels))
    padded[pl.ds(extent + 8, 8), :] = jnp.broadcast_to(edge[1:2], (8, channels))

    def widen(at, _):
        start = pl.multiple_of(at * BLOCK, BLOCK)
        padded[pl.ds(pl.multiple_of(start + 8, 8), BLOCK), :] = proj_ref[
            pl.ds(start, BLOCK), content : content + channels
        ].astype(jnp.float32)
        return 0

    lax.fori_loop(0, count, widen, 0)
    row = lax.broadcasted_iota(jnp.int32, (BLOCK, BLOCK), 0)
    column = lax.broadcasted_iota(jnp.int32, (BLOCK, BLOCK), 1)
    lower = (row >= column).astype(jnp.float32)
    upper = (row <= column).astype(jnp.float32)
    lane = lax.broadcasted_iota(jnp.int32, (1, LANES), 1)

    def block(at, _):
        start = pl.multiple_of(at * BLOCK, BLOCK)
        here = pl.ds(start, BLOCK)
        filtered = []
        for first in range(0, channels, 2 * LANES):
            part = padded[pl.ds(start, BLOCK + 16), first : first + 2 * LANES]
            taps = taps_ref[:, first : first + 2 * LANES]
            mixed = (
                taps[0:1] * part[7 : 7 + BLOCK]
                + taps[1:2] * part[8 : 8 + BLOCK]
                + taps[2:3] * part[9 : 9 + BLOCK]
            )
            filtered.append((mixed * sigmoid(mixed)).astype(jnp.bfloat16))
        filtered = jnp.concatenate(filtered, axis=1)
        signal = filtered[:, :content]
        inward = filtered[:, content : content + state_width]
        signal_ref[here, :] = signal
        inward_ref[here, :] = inward
        outward_ref[here, :] = filtered[:, content + state_width :]
        raw = proj_ref[here, content + channels :].astype(jnp.float32)
        steps = softplus(raw + offset_ref[...] - shift)
        logs = -steps * rate_ref[...]
        ahead = jnp.dot(lower, logs, precision=HIGHEST, preferred_element_type=jnp.float32)
        behind = jnp.dot(upper, logs, precision=HIGHEST, preferred_element_type=jnp.float32)
        within = jnp.where(lane < heads, ahead, behind)
        final = jnp.where(lane < heads, within[BLOCK - 1 : BLOCK], within[0:1])
        within_ref[here, :] = within
        rows_ref[0 : 2 * heads, here] = within.T[0 : 2 * heads]
        rows_ref[2 * heads : 4 * heads, here] = steps.T[0 : 2 * heads]
        scale = jnp.exp(final - within) * steps
        for group in range(groups):
            wide = signal[:, group * span : (group + 1) * span].astype(jnp.float32)
            scaled = jnp.concatenate(
                [wide * spread(scale, way * heads + group * ratio, ratio) for way in range(2)],
                axis=1,
            ).astype(jnp.bfloat16)
            added = lax.dot_general(
                inward[:, group * STATE : (group + 1) * STATE],
                scaled,
                (((0,), (0,)), ((), ())),
                preferred_element_type=jnp.float32,
            )
            block_states_ref[group, at] = added
            block_logs_ref[group, at] = jnp.concatenate(
                [spread(final, way * heads + group * ratio, ratio) for way in range(2)], axis=1
            )
        return 0

    lax.fori_loop(0, count, block, 0)
    logs_total[...] = jnp.zeros_like(logs_total)
    for group in range(groups):

        def onward(at, state):
            return state * jnp.exp(block_logs_ref[group, at][:, :span]) + block_states_ref[
                group, at
            ][:, :span]

        def back(at, state):
            at = count - 1 - at
            return state * jnp.exp(block_logs_ref[group, at][:, span:]) + block_states_ref[
                group, at
            ][:, span:]

        def total(at, carried):
            return carried + block_logs_ref[group, at]

        empty = jnp.zeros((STATE, span), jnp.float32)
        here = slice(group * STATE, (group + 1) * STATE)
        sent_ref[0, here, :] = lax.fori_loop(0, count, onward, empty).astype(jnp.bfloat16)
        sent_ref[1, here, :] = lax.fori_loop(0, count, back, empty).astype(jnp.bfloat16)
        decayed = lax.fori_loop(0, count, total, jnp.zeros((1, 2 * span), jnp.float32))
        coarse = decayed.astype(jnp.bfloat16).astype(jnp.float32)
        logs_total[2 * group : 2 * group + 1, :] = coarse
        logs_total[2 * group + 1 : 2 * group + 2, :] = decayed - coarse
    for way in range(2):
        sent_ref[way, groups * STATE :, :] = logs_total[:, way * span : (way + 1) * span].astype(
            jnp.bfloat16
        )


def diagonal_kernel(shape, signal_ref, inward_ref, outward_ref, within_ref, rows_ref, result_ref):
    groups, ratio, heads = shape
    count = signal_ref.shape[0] // BLOCK
    row = lax.broadcasted_iota(jnp.int32, (BLOCK, BLOCK), 0)
    column = lax.broadcasted_iota(jnp.int32, (BLOCK, BLOCK), 1)
    lane = lax.broadcasted_iota(jnp.int32, (BLOCK, LANES), 1)

    def block(at, _):
        here = pl.ds(pl.multiple_of(at * BLOCK, BLOCK), BLOCK)
        within = within_ref[here, :]
        for group in range(groups):
            intersect = lax.dot_general(
                outward_ref[here, group * STATE : (group + 1) * STATE],
                inward_ref[here, group * STATE : (group + 1) * STATE],
                (((1,), (1,)), ((), ())),
                preferred_element_type=jnp.float32,
            )
            products = []
            for head in range(group * ratio, (group + 1) * ratio):
                other = heads + head
                gap_ahead = within[:, head : head + 1] - rows_ref[head : head + 1, here]
                gap_behind = within[:, other : other + 1] - rows_ref[other : other + 1, here]
                step_ahead = rows_ref[2 * heads + head : 2 * heads + head + 1, here]
                step_behind = rows_ref[2 * heads + other : 2 * heads + other + 1, here]
                gap = jnp.where(row >= column, gap_ahead, gap_behind)
                step = jnp.where(
                    row > column,
                    step_ahead,
                    jnp.where(row < column, step_behind, step_ahead + step_behind),
                )
                weights = (intersect * jnp.exp(gap) * step).astype(jnp.bfloat16)
                tile = head // 2 * 2 * HEAD_DIM
                products.append(
                    jnp.dot(
                        weights,
                        signal_ref[here, tile : tile + LANES],
                        preferred_element_type=jnp.float32,
                    )
                )
            for pair in range(ratio // 2):
                at_tile = (group * ratio + 2 * pair) * HEAD_DIM
                result_ref[here, at_tile : at_tile + LANES] = jnp.where(
                    lane < HEAD_DIM, products[2 * pair], products[2 * pair + 1]
                )
        return 0

    lax.fori_loop(0, count, block, 0)


def finish_kernel(
    shape,
    gathered_ref,
    block_states_ref,
    block_logs_ref,
    outward_ref,
    within_ref,
    diagonal_ref,
    proj_ref,
    gain_ref,
    mixed_ref,
    total,
):
    groups, ratio, heads = shape
    stretches = gathered_ref.shape[0]
    count = outward_ref.shape[0] // BLOCK
    span = ratio * HEAD_DIM
    me = lax.axis_index("sp")
    for group in range(groups):
        states = slice(group * STATE, (group + 1) * STATE)
        log_at = groups * STATE

        def incoming(source, state):
            logs = gathered_ref[source, log_at : log_at + 16, :].astype(jnp.float32)
            logs = logs[2 * group : 2 * group + 1] + logs[2 * group + 1 : 2 * group + 2]
            return state * jnp.exp(logs) + gathered_ref[source, states, :].astype(jnp.float32)

        empty = jnp.zeros((STATE, span), jnp.float32)
        ahead = lax.fori_loop(0, me, incoming, empty)
        behind = lax.fori_loop(
            0,
            stretches - 1 - me,
            lambda hop, state: incoming(stretches - 1 - hop, state),
            empty,
        )
        wide = slice(group * span, (group + 1) * span)

        def back(hop, state):
            at = count - 1 - hop
            here = pl.ds(pl.multiple_of(at * BLOCK, BLOCK), BLOCK)
            carried = jnp.dot(
                outward_ref[here, states],
                state.astype(jnp.bfloat16),
                preferred_element_type=jnp.float32,
            )
            decay = spread(jnp.exp(within_ref[here, :]), heads + group * ratio, ratio)
            total[here, wide] = diagonal_ref[here, wide] + carried * decay
            return (
                state * jnp.exp(block_logs_ref[group, at][:, span:])
                + block_states_ref[group, at][:, span:]
            )

        lax.fori_loop(0, count, back, behind)

        def onward(at, state):
            here = pl.ds(pl.multiple_of(at * BLOCK, BLOCK), BLOCK)
            carried = jnp.dot(
                outward_ref[here, states],
                state.astype(jnp.bfloat16),
                preferred_element_type=jnp.float32,
            )
            decay = spread(jnp.exp(within_ref[here, :]), group * ratio, ratio)
            gate = proj_ref[here, wide].astype(jnp.float32)
            gated = (total[here, wide] + carried * decay) * (gate * sigmoid(gate))
            scale = lax.rsqrt(jnp.mean(gated * gated, axis=-1, keepdims=True) + EPSILON)
            mixed_ref[here, wide] = (gated * scale * gain_ref[:, wide]).astype(jnp.bfloat16)
            return (
                state * jnp.exp(block_logs_ref[group, at][:, :span])
                + block_states_ref[group, at][:, :span]
            )

        lax.fori_loop(0, count, onward, ahead)


def ring_place(index, count):
    outer, inner = index // 2, index % 2
    return (1 - inner) * outer + inner * (count - 1 - outer)


def ring_index(place, count):
    far = place // (count // 2)
    return (1 - far) * (2 * place) + far * (2 * (count - 1 - place) + 1)


def greet(peers):
    barrier = pltpu.get_barrier_semaphore()
    for peer in peers:
        pl.semaphore_signal(
            barrier, inc=1, device_id=peer, device_id_type=pl.DeviceIdType.MESH
        )
    pl.semaphore_wait(barrier, len(peers))


def remote(source, target, send, receive, peer):
    return pltpu.make_async_remote_copy(
        src_ref=source,
        dst_ref=target,
        send_sem=send,
        recv_sem=receive,
        device_id=peer,
        device_id_type=pl.DeviceIdType.MESH,
    )


def gather_kernel(
    stretches,
    parts,
    tokens_ref,
    weights_ref,
    all_tokens_ref,
    all_weights_ref,
    token_send,
    token_receive,
    ring_send,
    ring_receive,
    own,
):
    me, part = lax.axis_index("sp"), lax.axis_index("tp")
    place = ring_place(me, stretches)
    half_rows = weights_ref.shape[0] // 2
    right = (ring_index((place + 1) % stretches, stretches), part)
    left = (ring_index((place + stretches - 1) % stretches, stretches), part)
    across = [(me, (part + hop) % parts) for hop in range(1, parts)]
    greet([right, left] + across)
    sends = []
    for hop, peer in enumerate(across):
        copy = remote(
            tokens_ref, all_tokens_ref.at[part], token_send.at[hop], token_receive.at[hop], peer
        )
        copy.start()
        sends.append(copy)
    kept = [
        pltpu.make_async_copy(tokens_ref, all_tokens_ref.at[part], own.at[0]),
        pltpu.make_async_copy(weights_ref, all_weights_ref.at[me], own.at[1]),
    ]
    ring_sends = []
    for hop in range(stretches // 2):
        arriving = []
        for way, peer in enumerate((right, left)):
            source = ring_index((place + stretches + (2 * way - 1) * hop) % stretches, stretches)
            taken = weights_ref if hop == 0 else all_weights_ref.at[source]
            landed = all_weights_ref.at[source]
            if hop == stretches // 2 - 1:
                rows = pl.ds(way * half_rows, half_rows)
                taken, landed = taken.at[rows], landed.at[rows]
            copy = remote(
                taken, landed, ring_send.at[way, hop], ring_receive.at[way, hop], peer
            )
            copy.start()
            arriving.append(copy)
        if hop == 0:
            for copy in kept:
                copy.start()
        for copy in arriving:
            copy.wait_recv()
        ring_sends += arriving
    for copy in sends:
        copy.wait()
    for copy in ring_sends:
        copy.wait_send()
    for copy in kept:
        copy.wait()


def exchange_kernel(stretches, sent_ref, gathered_ref, send, receive):
    me, part = lax.axis_index("sp"), lax.axis_index("tp")
    peers = [(me + hop) % stretches for hop in range(1, stretches)]
    greet([(peer, part) for peer in peers])
    copies = []
    for hop, peer in enumerate(peers):
        wrapped = (me + hop + 1) // stretches
        copy = remote(
            sent_ref.at[wrapped],
            gathered_ref.at[me],
            send.at[hop],
            receive.at[hop],
            (peer, part),
        )
        copy.start()
        copies.append(copy)
    for copy in copies:
        copy.wait()


def remote_call(body, out_shape, inputs, scratch, collective_id):
    space = pl.BlockSpec(memory_space=pltpu.VMEM)
    return pl.pallas_call(
        body,
        out_shape=out_shape,
        in_specs=[space] * inputs,
        out_specs=jax.tree.map(lambda _: space, out_shape),
        scratch_shapes=scratch,
        cost_estimate=pl.CostEstimate(
            flops=int(3e10), bytes_accessed=1 << 20, transcendentals=0
        ),
        compiler_params=pltpu.CompilerParams(
            collective_id=collective_id, has_side_effects=True, vmem_limit_bytes=VMEM_LIMIT
        ),
    )


def kernel_call(body, out_shape, scratch, micros):
    return pl.pallas_call(
        body,
        out_shape=out_shape,
        scratch_shapes=scratch,
        cost_estimate=pl.CostEstimate(
            flops=int(micros * 5e8), bytes_accessed=1 << 20, transcendentals=0
        ),
        compiler_params=pltpu.CompilerParams(vmem_limit_bytes=VMEM_LIMIT),
    )


def on_device(
    input_activations,
    norm_gain,
    w_gate,
    w_value,
    w_state_in,
    w_state_out,
    w_step_forward,
    w_step_backward,
    step_offset,
    fading_speed,
    conv_value,
    conv_state_in,
    conv_state_out,
    out_gain,
    w_out,
):
    stretches = lax.axis_size("sp")
    content = w_value.shape[1]
    state_width = w_state_in.shape[1]
    heads = w_step_forward.shape[1]
    groups = state_width // STATE
    ratio = heads // groups
    span = ratio * HEAD_DIM
    channels = content + 2 * state_width
    depth = w_gate.shape[0]
    spare = -2 * heads % LANES

    weights = jnp.concatenate(
        [
            w_gate,
            w_value,
            w_state_in,
            w_state_out,
            w_step_forward,
            w_step_backward,
            jnp.zeros((depth, spare), w_gate.dtype),
        ],
        axis=1,
    )
    normed = (rms_rows(input_activations) * norm_gain).astype(jnp.bfloat16)
    parts = lax.axis_size("tp")
    dma = pltpu.SemaphoreType.DMA
    tokens, all_weights = remote_call(
        functools.partial(gather_kernel, stretches, parts),
        (
            jax.ShapeDtypeStruct((parts, *normed.shape), normed.dtype),
            jax.ShapeDtypeStruct((stretches, *weights.shape), weights.dtype),
        ),
        2,
        [
            dma((parts - 1,)),
            dma((parts - 1,)),
            dma((2, stretches // 2)),
            dma((2, stretches // 2)),
            dma((2,)),
        ],
        1,
    )(normed, weights)
    tokens, all_weights, w_out = lax.optimization_barrier((tokens, all_weights, w_out))
    tokens = tokens.reshape(-1, tokens.shape[2])
    all_weights = all_weights.reshape(-1, all_weights.shape[2])
    full_out = lax.all_gather(w_out, "sp", axis=1, tiled=True)
    proj = jnp.dot(tokens, all_weights, preferred_element_type=jnp.float32).astype(jnp.bfloat16)
    extent = tokens.shape[0]
    count = extent // BLOCK

    onward = [(i, i + 1) for i in range(stretches - 1)]
    back = [(target, source) for source, target in onward]
    low = lax.ppermute(proj[extent - 1 :, content : content + channels], "sp", onward)
    high = lax.ppermute(proj[:1, content : content + channels], "sp", back)
    edges = jnp.concatenate([low, high], axis=0)

    taps = jnp.concatenate([conv_value, conv_state_in, conv_state_out], axis=1)
    padding = ((0, 0), (0, spare))
    offset = jnp.pad(step_offset.reshape(1, 2 * heads), padding)
    rate = jnp.pad(fading_speed.reshape(1, 2 * heads), padding)
    shift = math.log(extent * stretches)

    bf16, f32 = jnp.bfloat16, jnp.float32
    made = jax.ShapeDtypeStruct
    sent_rows = groups * STATE + 16
    signal, inward, outward, within, rows, block_states, block_logs, sent = kernel_call(
        functools.partial(states_kernel, (groups, ratio, content, state_width, heads, shift)),
        (
            made((extent, content), bf16),
            made((extent, state_width), bf16),
            made((extent, state_width), bf16),
            made((extent, LANES), f32),
            made((4 * heads, extent), f32),
            made((groups, count, STATE, 2 * span), f32),
            made((groups, count, 1, 2 * span), f32),
            made((2, sent_rows, span), bf16),
        ),
        [pltpu.VMEM((extent + 16, channels), f32), pltpu.VMEM((16, 2 * span), f32)],
        15,
    )(proj, edges, taps, offset, rate)
    gathered = remote_call(
        functools.partial(exchange_kernel, stretches),
        made((stretches, sent_rows, span), bf16),
        1,
        [dma((stretches - 1,)), dma((stretches - 1,))],
        2,
    )(sent)
    diagonal = kernel_call(
        functools.partial(diagonal_kernel, (groups, ratio, heads)),
        made((extent, content), f32),
        [],
        15,
    )(signal, inward, outward, within, rows)
    mixed = kernel_call(
        functools.partial(finish_kernel, (groups, ratio, heads)),
        made((extent, content), bf16),
        [pltpu.VMEM((extent, content), f32)],
        15,
    )(
        gathered,
        block_states,
        block_logs,
        outward,
        within,
        diagonal,
        proj,
        out_gain.reshape(1, content),
    )
    partial = jnp.dot(mixed, full_out, preferred_element_type=jnp.float32).astype(jnp.bfloat16)
    return lax.psum_scatter(partial, "tp", scatter_dimension=0, tiled=True)


def solution(mesh):
    return jax.shard_map(
        on_device,
        mesh=mesh,
        in_specs=(
            P(("sp", "tp"), None),
            P(),
            P("sp", "tp"),
            P("sp", "tp"),
            P("sp", "tp"),
            P("sp", "tp"),
            P("sp", "tp"),
            P("sp", "tp"),
            P(None, "tp"),
            P(None, "tp"),
            P(None, "tp"),
            P(None, "tp"),
            P(None, "tp"),
            P("tp"),
            P("tp", "sp"),
        ),
        out_specs=P(("sp", "tp"), None),
        check_vma=False,
    )
```

```python
import functools
import math

import jax
import jax.numpy as jnp
from jax import lax
from jax.experimental import pallas as pl
from jax.experimental.pallas import tpu as pltpu
from jax.sharding import PartitionSpec as P

HEAD_DIM = 64
STATE = 128
BLOCK = 128
LANES = 128
EPSILON = 1e-06
HIGHEST = lax.Precision.HIGHEST
VMEM_LIMIT = 60 * 1024 * 1024


def rms_rows(values):
    wide = values.astype(jnp.float32)
    return wide * lax.rsqrt(jnp.mean(wide * wide, axis=-1, keepdims=True) + EPSILON)


def sigmoid(values):
    return 1.0 / (1.0 + jnp.exp(-values))


def softplus(values):
    return jnp.maximum(values, 0.0) + jnp.log1p(jnp.exp(-jnp.abs(values)))


def spread(columns, first, count):
    rows = columns.shape[0]
    lane = lax.broadcasted_iota(jnp.int32, (rows, LANES), 1)
    tiles = []
    for at in range(first, first + count, 2):
        low = jnp.broadcast_to(columns[:, at : at + 1], (rows, LANES))
        high = jnp.broadcast_to(columns[:, at + 1 : at + 2], (rows, LANES))
        tiles.append(jnp.where(lane < HEAD_DIM, low, high))
    return jnp.concatenate(tiles, axis=1)


def states_kernel(
    shape,
    proj_ref,
    edges_ref,
    taps_ref,
    offset_ref,
    rate_ref,
    signal_ref,
    inward_ref,
    outward_ref,
    within_ref,
    rows_ref,
    block_states_ref,
    block_logs_ref,
    sent_ref,
    padded,
    logs_total,
):
    groups, ratio, content, state_width, heads, shift = shape
    extent = proj_ref.shape[0]
    count = extent // BLOCK
    channels = content + 2 * state_width
    span = ratio * HEAD_DIM
    edge = edges_ref[...].astype(jnp.float32)
    padded[pl.ds(0, 8), :] = jnp.broadcast_to(edge[0:1], (8, channels))
    padded[pl.ds(extent + 8, 8), :] = jnp.broadcast_to(edge[1:2], (8, channels))

    def widen(at, _):
        start = pl.multiple_of(at * BLOCK, BLOCK)
        padded[pl.ds(pl.multiple_of(start + 8, 8), BLOCK), :] = proj_ref[
            pl.ds(start, BLOCK), content : content + channels
        ].astype(jnp.float32)
        return 0

    lax.fori_loop(0, count, widen, 0)
    row = lax.broadcasted_iota(jnp.int32, (BLOCK, BLOCK), 0)
    column = lax.broadcasted_iota(jnp.int32, (BLOCK, BLOCK), 1)
    lower = (row >= column).astype(jnp.float32)
    upper = (row <= column).astype(jnp.float32)
    lane = lax.broadcasted_iota(jnp.int32, (1, LANES), 1)

    def block(at, _):
        start = pl.multiple_of(at * BLOCK, BLOCK)
        here = pl.ds(start, BLOCK)
        filtered = []
        for first in range(0, channels, 2 * LANES):
            part = padded[pl.ds(start, BLOCK + 16), first : first + 2 * LANES]
            taps = taps_ref[:, first : first + 2 * LANES]
            mixed = (
                taps[0:1] * part[7 : 7 + BLOCK]
                + taps[1:2] * part[8 : 8 + BLOCK]
                + taps[2:3] * part[9 : 9 + BLOCK]
            )
            filtered.append((mixed * sigmoid(mixed)).astype(jnp.bfloat16))
        filtered = jnp.concatenate(filtered, axis=1)
        signal = filtered[:, :content]
        inward = filtered[:, content : content + state_width]
        signal_ref[here, :] = signal
        inward_ref[here, :] = inward
        outward_ref[here, :] = filtered[:, content + state_width :]
        raw = proj_ref[here, content + channels :].astype(jnp.float32)
        steps = softplus(raw + offset_ref[...] - shift)
        logs = -steps * rate_ref[...]
        ahead = jnp.dot(lower, logs, precision=HIGHEST, preferred_element_type=jnp.float32)
        behind = jnp.dot(upper, logs, precision=HIGHEST, preferred_element_type=jnp.float32)
        within = jnp.where(lane < heads, ahead, behind)
        final = jnp.where(lane < heads, within[BLOCK - 1 : BLOCK], within[0:1])
        within_ref[here, :] = within
        rows_ref[0 : 2 * heads, here] = within.T[0 : 2 * heads]
        rows_ref[2 * heads : 4 * heads, here] = steps.T[0 : 2 * heads]
        scale = jnp.exp(final - within) * steps
        for group in range(groups):
            wide = signal[:, group * span : (group + 1) * span].astype(jnp.float32)
            scaled = jnp.concatenate(
                [wide * spread(scale, way * heads + group * ratio, ratio) for way in range(2)],
                axis=1,
            ).astype(jnp.bfloat16)
            added = lax.dot_general(
                inward[:, group * STATE : (group + 1) * STATE],
                scaled,
                (((0,), (0,)), ((), ())),
                preferred_element_type=jnp.float32,
            )
            block_states_ref[group, at] = added
            block_logs_ref[group, at] = jnp.concatenate(
                [spread(final, way * heads + group * ratio, ratio) for way in range(2)], axis=1
            )
        return 0

    lax.fori_loop(0, count, block, 0)
    logs_total[...] = jnp.zeros_like(logs_total)
    for group in range(groups):

        def onward(at, state):
            return state * jnp.exp(block_logs_ref[group, at][:, :span]) + block_states_ref[
                group, at
            ][:, :span]

        def back(at, state):
            at = count - 1 - at
            return state * jnp.exp(block_logs_ref[group, at][:, span:]) + block_states_ref[
                group, at
            ][:, span:]

        def total(at, carried):
            return carried + block_logs_ref[group, at]

        empty = jnp.zeros((STATE, span), jnp.float32)
        here = slice(group * STATE, (group + 1) * STATE)
        sent_ref[0, here, :] = lax.fori_loop(0, count, onward, empty).astype(jnp.bfloat16)
        sent_ref[1, here, :] = lax.fori_loop(0, count, back, empty).astype(jnp.bfloat16)
        decayed = lax.fori_loop(0, count, total, jnp.zeros((1, 2 * span), jnp.float32))
        coarse = decayed.astype(jnp.bfloat16).astype(jnp.float32)
        logs_total[2 * group : 2 * group + 1, :] = coarse
        logs_total[2 * group + 1 : 2 * group + 2, :] = decayed - coarse
    for way in range(2):
        sent_ref[way, groups * STATE :, :] = logs_total[:, way * span : (way + 1) * span].astype(
            jnp.bfloat16
        )


def diagonal_kernel(shape, signal_ref, inward_ref, outward_ref, within_ref, rows_ref, result_ref):
    groups, ratio, heads = shape
    count = signal_ref.shape[0] // BLOCK
    row = lax.broadcasted_iota(jnp.int32, (BLOCK, BLOCK), 0)
    column = lax.broadcasted_iota(jnp.int32, (BLOCK, BLOCK), 1)
    lane = lax.broadcasted_iota(jnp.int32, (BLOCK, LANES), 1)

    def block(at, _):
        here = pl.ds(pl.multiple_of(at * BLOCK, BLOCK), BLOCK)
        within = within_ref[here, :]
        for group in range(groups):
            intersect = lax.dot_general(
                outward_ref[here, group * STATE : (group + 1) * STATE],
                inward_ref[here, group * STATE : (group + 1) * STATE],
                (((1,), (1,)), ((), ())),
                preferred_element_type=jnp.float32,
            )
            products = []
            for head in range(group * ratio, (group + 1) * ratio):
                other = heads + head
                gap_ahead = within[:, head : head + 1] - rows_ref[head : head + 1, here]
                gap_behind = within[:, other : other + 1] - rows_ref[other : other + 1, here]
                step_ahead = rows_ref[2 * heads + head : 2 * heads + head + 1, here]
                step_behind = rows_ref[2 * heads + other : 2 * heads + other + 1, here]
                gap = jnp.where(row >= column, gap_ahead, gap_behind)
                step = jnp.where(
                    row > column,
                    step_ahead,
                    jnp.where(row < column, step_behind, step_ahead + step_behind),
                )
                weights = (intersect * jnp.exp(gap) * step).astype(jnp.bfloat16)
                tile = head // 2 * 2 * HEAD_DIM
                products.append(
                    jnp.dot(
                        weights,
                        signal_ref[here, tile : tile + LANES],
                        preferred_element_type=jnp.float32,
                    )
                )
            for pair in range(ratio // 2):
                at_tile = (group * ratio + 2 * pair) * HEAD_DIM
                result_ref[here, at_tile : at_tile + LANES] = jnp.where(
                    lane < HEAD_DIM, products[2 * pair], products[2 * pair + 1]
                )
        return 0

    lax.fori_loop(0, count, block, 0)


def finish_kernel(
    shape,
    gathered_ref,
    block_states_ref,
    block_logs_ref,
    outward_ref,
    within_ref,
    diagonal_ref,
    proj_ref,
    gain_ref,
    mixed_ref,
    total,
):
    groups, ratio, heads = shape
    stretches = gathered_ref.shape[0]
    count = outward_ref.shape[0] // BLOCK
    span = ratio * HEAD_DIM
    me = lax.axis_index("sp")
    for group in range(groups):
        states = slice(group * STATE, (group + 1) * STATE)
        log_at = groups * STATE

        def incoming(source, state):
            logs = gathered_ref[source, log_at : log_at + 16, :].astype(jnp.float32)
            logs = logs[2 * group : 2 * group + 1] + logs[2 * group + 1 : 2 * group + 2]
            return state * jnp.exp(logs) + gathered_ref[source, states, :].astype(jnp.float32)

        empty = jnp.zeros((STATE, span), jnp.float32)
        ahead = lax.fori_loop(0, me, incoming, empty)
        behind = lax.fori_loop(
            0,
            stretches - 1 - me,
            lambda hop, state: incoming(stretches - 1 - hop, state),
            empty,
        )
        wide = slice(group * span, (group + 1) * span)

        def back(hop, state):
            at = count - 1 - hop
            here = pl.ds(pl.multiple_of(at * BLOCK, BLOCK), BLOCK)
            carried = jnp.dot(
                outward_ref[here, states],
                state.astype(jnp.bfloat16),
                preferred_element_type=jnp.float32,
            )
            decay = spread(jnp.exp(within_ref[here, :]), heads + group * ratio, ratio)
            total[here, wide] = diagonal_ref[here, wide] + carried * decay
            return (
                state * jnp.exp(block_logs_ref[group, at][:, span:])
                + block_states_ref[group, at][:, span:]
            )

        lax.fori_loop(0, count, back, behind)

        def onward(at, state):
            here = pl.ds(pl.multiple_of(at * BLOCK, BLOCK), BLOCK)
            carried = jnp.dot(
                outward_ref[here, states],
                state.astype(jnp.bfloat16),
                preferred_element_type=jnp.float32,
            )
            decay = spread(jnp.exp(within_ref[here, :]), group * ratio, ratio)
            gate = proj_ref[here, wide].astype(jnp.float32)
            gated = (total[here, wide] + carried * decay) * (gate * sigmoid(gate))
            scale = lax.rsqrt(jnp.mean(gated * gated, axis=-1, keepdims=True) + EPSILON)
            mixed_ref[here, wide] = (gated * scale * gain_ref[:, wide]).astype(jnp.bfloat16)
            return (
                state * jnp.exp(block_logs_ref[group, at][:, :span])
                + block_states_ref[group, at][:, :span]
            )

        lax.fori_loop(0, count, onward, ahead)


def ring_place(index, count):
    outer, inner = index // 2, index % 2
    return (1 - inner) * outer + inner * (count - 1 - outer)


def ring_index(place, count):
    far = place // (count // 2)
    return (1 - far) * (2 * place) + far * (2 * (count - 1 - place) + 1)


def greet(peers):
    barrier = pltpu.get_barrier_semaphore()
    for peer in peers:
        pl.semaphore_signal(
            barrier, inc=1, device_id=peer, device_id_type=pl.DeviceIdType.MESH
        )
    pl.semaphore_wait(barrier, len(peers))


def remote(source, target, send, receive, peer):
    return pltpu.make_async_remote_copy(
        src_ref=source,
        dst_ref=target,
        send_sem=send,
        recv_sem=receive,
        device_id=peer,
        device_id_type=pl.DeviceIdType.MESH,
    )


def gather_kernel(
    stretches,
    parts,
    tokens_ref,
    weights_ref,
    all_tokens_ref,
    all_weights_ref,
    token_send,
    token_receive,
    ring_send,
    ring_receive,
    own,
):
    me, part = lax.axis_index("sp"), lax.axis_index("tp")
    place = ring_place(me, stretches)
    half_rows = weights_ref.shape[0] // 2
    right = (ring_index((place + 1) % stretches, stretches), part)
    left = (ring_index((place + stretches - 1) % stretches, stretches), part)
    across = [(me, (part + hop) % parts) for hop in range(1, parts)]
    greet([right, left] + across)
    sends = []
    for hop, peer in enumerate(across):
        copy = remote(
            tokens_ref, all_tokens_ref.at[part], token_send.at[hop], token_receive.at[hop], peer
        )
        copy.start()
        sends.append(copy)
    kept = [
        pltpu.make_async_copy(tokens_ref, all_tokens_ref.at[part], own.at[0]),
        pltpu.make_async_copy(weights_ref, all_weights_ref.at[me], own.at[1]),
    ]
    ring_sends = []
    for hop in range(stretches // 2):
        arriving = []
        for way, peer in enumerate((right, left)):
            source = ring_index((place + stretches + (2 * way - 1) * hop) % stretches, stretches)
            taken = weights_ref if hop == 0 else all_weights_ref.at[source]
            landed = all_weights_ref.at[source]
            if hop == stretches // 2 - 1:
                rows = pl.ds(way * half_rows, half_rows)
                taken, landed = taken.at[rows], landed.at[rows]
            copy = remote(
                taken, landed, ring_send.at[way, hop], ring_receive.at[way, hop], peer
            )
            copy.start()
            arriving.append(copy)
        if hop == 0:
            for copy in kept:
                copy.start()
        for copy in arriving:
            copy.wait_recv()
        ring_sends += arriving
    for copy in sends:
        copy.wait()
    for copy in ring_sends:
        copy.wait_send()
    for copy in kept:
        copy.wait()


def exchange_kernel(
    stretches,
    shape,
    sent_ref,
    signal_ref,
    inward_ref,
    outward_ref,
    within_ref,
    rows_ref,
    gathered_ref,
    result_ref,
    send,
    receive,
):
    me, part = lax.axis_index("sp"), lax.axis_index("tp")
    peers = [(me + hop) % stretches for hop in range(1, stretches)]
    greet([(peer, part) for peer in peers])
    copies = []
    for hop, peer in enumerate(peers):
        wrapped = (me + hop + 1) // stretches
        copy = remote(
            sent_ref.at[wrapped],
            gathered_ref.at[me],
            send.at[hop],
            receive.at[hop],
            (peer, part),
        )
        copy.start()
        copies.append(copy)
    diagonal_kernel(
        shape, signal_ref, inward_ref, outward_ref, within_ref, rows_ref, result_ref
    )
    for copy in copies:
        copy.wait()


def output_kernel(
    mixed_ref,
    weights_ref,
    result_ref,
    near_out,
    near_in,
    far_out,
    far_in,
    own,
    near_send,
    near_receive,
    far_send,
    far_receive,
):
    me, part = lax.axis_index("sp"), lax.axis_index("tp")
    pair, place = part // 2, part % 2
    near = (me, 2 * pair + 1 - place)
    far = (me, 2 * (1 - pair) + place)
    greet([near, far])
    extent = result_ref.shape[0]
    piece = extent // 2
    width = 4 * LANES

    def product(block, at, store):
        start = pl.multiple_of(block * extent + at * piece, piece)
        rows = mixed_ref[pl.ds(start, piece), :]

        def tile(step, _):
            columns = pl.ds(pl.multiple_of(step * width, width), width)
            total = jnp.dot(rows, weights_ref[:, columns], preferred_element_type=jnp.float32)
            store(columns, total)
            return 0

        lax.fori_loop(0, result_ref.shape[1] // width, tile, 0)

    def rows_of(at):
        return pl.ds(at * piece, piece)

    def to_near(block, turn, at):
        def store(columns, total):
            near_out[turn, rows_of(at), columns] = total.astype(jnp.bfloat16)

        product(block, at, store)
        return remote(
            near_out.at[turn, rows_of(at)],
            near_in.at[turn, rows_of(at)],
            near_send.at[turn, at],
            near_receive.at[turn, at],
            near,
        )

    def to_far(block, at, arriving):
        arriving.wait_recv()

        def store(columns, total):
            total = total + near_in[0, rows_of(at), columns].astype(jnp.float32)
            far_out[rows_of(at), columns] = total.astype(jnp.bfloat16)

        product(block, at, store)
        return remote(
            far_out.at[rows_of(at)],
            far_in.at[rows_of(at)],
            far_send.at[at],
            far_receive.at[at],
            far,
        )

    def keep(at):
        def store(columns, total):
            own[rows_of(at), columns] = total

        product(part, at, store)

    theirs, mine = 2 * (1 - pair) + 1 - place, 2 * (1 - pair) + place
    first = [to_near(theirs, 0, 0), None]
    first[1] = to_near(theirs, 0, 1)
    first[0].start()
    keep(0)
    first[1].start()
    keep(1)
    across = [to_far(mine, 0, first[0]), None]
    across[1] = to_far(mine, 1, first[1])
    across[0].start()
    second = [to_near(2 * pair + 1 - place, 1, 0), None]
    across[1].start()
    second[1] = to_near(2 * pair + 1 - place, 1, 1)
    second[0].start()
    second[0].wait_recv()
    own[rows_of(0), :] += near_in[1, rows_of(0), :].astype(jnp.float32)
    second[1].start()
    second[1].wait_recv()
    own[rows_of(1), :] += near_in[1, rows_of(1), :].astype(jnp.float32)
    for at in range(2):
        across[at].wait_recv()
        total = own[rows_of(at), :] + far_in[rows_of(at), :].astype(jnp.float32)
        result_ref[rows_of(at), :] = total.astype(result_ref.dtype)
    for copy in first + second + across:
        copy.wait_send()


def remote_call(body, out_shape, inputs, scratch, collective_id):
    space = pl.BlockSpec(memory_space=pltpu.VMEM)
    return pl.pallas_call(
        body,
        out_shape=out_shape,
        in_specs=[space] * inputs,
        out_specs=jax.tree.map(lambda _: space, out_shape),
        scratch_shapes=scratch,
        cost_estimate=pl.CostEstimate(
            flops=int(3e10), bytes_accessed=1 << 20, transcendentals=0
        ),
        compiler_params=pltpu.CompilerParams(
            collective_id=collective_id, has_side_effects=True, vmem_limit_bytes=VMEM_LIMIT
        ),
    )


def kernel_call(body, out_shape, scratch, micros):
    return pl.pallas_call(
        body,
        out_shape=out_shape,
        scratch_shapes=scratch,
        cost_estimate=pl.CostEstimate(
            flops=int(micros * 5e8), bytes_accessed=1 << 20, transcendentals=0
        ),
        compiler_params=pltpu.CompilerParams(vmem_limit_bytes=VMEM_LIMIT),
    )


def on_device(
    input_activations,
    norm_gain,
    w_gate,
    w_value,
    w_state_in,
    w_state_out,
    w_step_forward,
    w_step_backward,
    step_offset,
    fading_speed,
    conv_value,
    conv_state_in,
    conv_state_out,
    out_gain,
    w_out,
):
    stretches = lax.axis_size("sp")
    content = w_value.shape[1]
    state_width = w_state_in.shape[1]
    heads = w_step_forward.shape[1]
    groups = state_width // STATE
    ratio = heads // groups
    span = ratio * HEAD_DIM
    channels = content + 2 * state_width
    depth = w_gate.shape[0]
    spare = -2 * heads % LANES

    weights = jnp.concatenate(
        [
            w_gate,
            w_value,
            w_state_in,
            w_state_out,
            w_step_forward,
            w_step_backward,
            jnp.zeros((depth, spare), w_gate.dtype),
        ],
        axis=1,
    )
    normed = (rms_rows(input_activations) * norm_gain).astype(jnp.bfloat16)
    parts = lax.axis_size("tp")
    dma = pltpu.SemaphoreType.DMA
    tokens, all_weights = remote_call(
        functools.partial(gather_kernel, stretches, parts),
        (
            jax.ShapeDtypeStruct((parts, *normed.shape), normed.dtype),
            jax.ShapeDtypeStruct((stretches, *weights.shape), weights.dtype),
        ),
        2,
        [
            dma((parts - 1,)),
            dma((parts - 1,)),
            dma((2, stretches // 2)),
            dma((2, stretches // 2)),
            dma((2,)),
        ],
        1,
    )(normed, weights)
    tokens, all_weights, w_out = lax.optimization_barrier((tokens, all_weights, w_out))
    tokens = tokens.reshape(-1, tokens.shape[2])
    all_weights = all_weights.reshape(-1, all_weights.shape[2])
    full_out = lax.all_gather(w_out, "sp", axis=1, tiled=True)
    proj = jnp.dot(tokens, all_weights, preferred_element_type=jnp.float32).astype(jnp.bfloat16)
    extent = tokens.shape[0]
    count = extent // BLOCK

    onward = [(i, i + 1) for i in range(stretches - 1)]
    back = [(target, source) for source, target in onward]
    low = lax.ppermute(proj[extent - 1 :, content : content + channels], "sp", onward)
    high = lax.ppermute(proj[:1, content : content + channels], "sp", back)
    edges = jnp.concatenate([low, high], axis=0)

    taps = jnp.concatenate([conv_value, conv_state_in, conv_state_out], axis=1)
    padding = ((0, 0), (0, spare))
    offset = jnp.pad(step_offset.reshape(1, 2 * heads), padding)
    rate = jnp.pad(fading_speed.reshape(1, 2 * heads), padding)
    shift = math.log(extent * stretches)

    bf16, f32 = jnp.bfloat16, jnp.float32
    made = jax.ShapeDtypeStruct
    sent_rows = groups * STATE + 16
    signal, inward, outward, within, rows, block_states, block_logs, sent = kernel_call(
        functools.partial(states_kernel, (groups, ratio, content, state_width, heads, shift)),
        (
            made((extent, content), bf16),
            made((extent, state_width), bf16),
            made((extent, state_width), bf16),
            made((extent, LANES), f32),
            made((4 * heads, extent), f32),
            made((groups, count, STATE, 2 * span), f32),
            made((groups, count, 1, 2 * span), f32),
            made((2, sent_rows, span), bf16),
        ),
        [pltpu.VMEM((extent + 16, channels), f32), pltpu.VMEM((16, 2 * span), f32)],
        15,
    )(proj, edges, taps, offset, rate)
    gathered, diagonal = remote_call(
        functools.partial(exchange_kernel, stretches, (groups, ratio, heads)),
        (made((stretches, sent_rows, span), bf16), made((extent, content), f32)),
        6,
        [dma((stretches - 1,)), dma((stretches - 1,))],
        2,
    )(sent, signal, inward, outward, within, rows)
    mixed = kernel_call(
        functools.partial(finish_kernel, (groups, ratio, heads)),
        made((extent, content), bf16),
        [pltpu.VMEM((extent, content), f32)],
        15,
    )(
        gathered,
        block_states,
        block_logs,
        outward,
        within,
        diagonal,
        proj,
        out_gain.reshape(1, content),
    )
    rows_out, features = input_activations.shape
    if parts != 4:
        partial = jnp.dot(mixed, full_out, preferred_element_type=f32).astype(bf16)
        return lax.psum_scatter(partial, "tp", scatter_dimension=0, tiled=True)
    return remote_call(
        output_kernel,
        made((rows_out, features), bf16),
        2,
        [
            pltpu.VMEM((2, rows_out, features), bf16),
            pltpu.VMEM((2, rows_out, features), bf16),
            pltpu.VMEM((rows_out, features), bf16),
            pltpu.VMEM((rows_out, features), bf16),
            pltpu.VMEM((rows_out, features), f32),
            dma((2, 2)),
            dma((2, 2)),
            dma((2,)),
            dma((2,)),
        ],
        3,
    )(mixed, full_out)


def solution(mesh):
    return jax.shard_map(
        on_device,
        mesh=mesh,
        in_specs=(
            P(("sp", "tp"), None),
            P(),
            P("sp", "tp"),
            P("sp", "tp"),
            P("sp", "tp"),
            P("sp", "tp"),
            P("sp", "tp"),
            P("sp", "tp"),
            P(None, "tp"),
            P(None, "tp"),
            P(None, "tp"),
            P(None, "tp"),
            P(None, "tp"),
            P("tp"),
            P("tp", "sp"),
        ),
        out_specs=P(("sp", "tp"), None),
        check_vma=False,
    )
```

```python
import functools
import math

import jax
import jax.numpy as jnp
from jax import lax
from jax.experimental import pallas as pl
from jax.experimental.pallas import tpu as pltpu
from jax.sharding import PartitionSpec as P

HEAD_DIM = 64
STATE = 128
BLOCK = 128
LANES = 128
EPSILON = 1e-06
HIGHEST = lax.Precision.HIGHEST
VMEM_LIMIT = 60 * 1024 * 1024


def rms_rows(values):
    wide = values.astype(jnp.float32)
    return wide * lax.rsqrt(jnp.mean(wide * wide, axis=-1, keepdims=True) + EPSILON)


def sigmoid(values):
    return 1.0 / (1.0 + jnp.exp(-values))


def softplus(values):
    return jnp.maximum(values, 0.0) + jnp.log1p(jnp.exp(-jnp.abs(values)))


def spread(columns, first, count):
    rows = columns.shape[0]
    lane = lax.broadcasted_iota(jnp.int32, (rows, LANES), 1)
    tiles = []
    for at in range(first, first + count, 2):
        low = jnp.broadcast_to(columns[:, at : at + 1], (rows, LANES))
        high = jnp.broadcast_to(columns[:, at + 1 : at + 2], (rows, LANES))
        tiles.append(jnp.where(lane < HEAD_DIM, low, high))
    return jnp.concatenate(tiles, axis=1)


def states_kernel(
    shape,
    proj_ref,
    edges_ref,
    taps_ref,
    offset_ref,
    rate_ref,
    signal_ref,
    inward_ref,
    outward_ref,
    within_ref,
    rows_ref,
    block_states_ref,
    block_logs_ref,
    sent_ref,
    padded,
    logs_total,
):
    groups, ratio, content, state_width, heads, shift = shape
    extent = proj_ref.shape[0]
    count = extent // BLOCK
    channels = content + 2 * state_width
    span = ratio * HEAD_DIM
    me, last = lax.axis_index("sp"), lax.axis_size("sp") - 1
    low = edges_ref[0, :, content : content + channels].astype(jnp.float32)
    high = edges_ref[1, :, content : content + channels].astype(jnp.float32)
    padded[pl.ds(0, 8), :] = jnp.where(me > 0, low[8:], 0.0)
    padded[pl.ds(extent + 8, 8), :] = jnp.where(me < last, high[:8], 0.0)

    def widen(at, _):
        start = pl.multiple_of(at * BLOCK, BLOCK)
        padded[pl.ds(pl.multiple_of(start + 8, 8), BLOCK), :] = proj_ref[
            pl.ds(start, BLOCK), content : content + channels
        ].astype(jnp.float32)
        return 0

    lax.fori_loop(0, count, widen, 0)
    row = lax.broadcasted_iota(jnp.int32, (BLOCK, BLOCK), 0)
    column = lax.broadcasted_iota(jnp.int32, (BLOCK, BLOCK), 1)
    lower = (row >= column).astype(jnp.float32)
    upper = (row <= column).astype(jnp.float32)
    lane = lax.broadcasted_iota(jnp.int32, (1, LANES), 1)

    def block(at, _):
        start = pl.multiple_of(at * BLOCK, BLOCK)
        here = pl.ds(start, BLOCK)
        filtered = []
        for first in range(0, channels, 2 * LANES):
            part = padded[pl.ds(start, BLOCK + 16), first : first + 2 * LANES]
            taps = taps_ref[:, first : first + 2 * LANES]
            mixed = (
                taps[0:1] * part[7 : 7 + BLOCK]
                + taps[1:2] * part[8 : 8 + BLOCK]
                + taps[2:3] * part[9 : 9 + BLOCK]
            )
            filtered.append((mixed * sigmoid(mixed)).astype(jnp.bfloat16))
        filtered = jnp.concatenate(filtered, axis=1)
        signal = filtered[:, :content]
        inward = filtered[:, content : content + state_width]
        signal_ref[here, :] = signal
        inward_ref[here, :] = inward
        outward_ref[here, :] = filtered[:, content + state_width :]
        raw = proj_ref[here, content + channels :].astype(jnp.float32)
        steps = softplus(raw + offset_ref[...] - shift)
        logs = -steps * rate_ref[...]
        ahead = jnp.dot(lower, logs, precision=HIGHEST, preferred_element_type=jnp.float32)
        behind = jnp.dot(upper, logs, precision=HIGHEST, preferred_element_type=jnp.float32)
        within = jnp.where(lane < heads, ahead, behind)
        final = jnp.where(lane < heads, within[BLOCK - 1 : BLOCK], within[0:1])
        within_ref[here, :] = within
        rows_ref[0 : 2 * heads, here] = within.T[0 : 2 * heads]
        rows_ref[2 * heads : 4 * heads, here] = steps.T[0 : 2 * heads]
        scale = jnp.exp(final - within) * steps
        for group in range(groups):
            wide = signal[:, group * span : (group + 1) * span].astype(jnp.float32)
            scaled = jnp.concatenate(
                [wide * spread(scale, way * heads + group * ratio, ratio) for way in range(2)],
                axis=1,
            ).astype(jnp.bfloat16)
            added = lax.dot_general(
                inward[:, group * STATE : (group + 1) * STATE],
                scaled,
                (((0,), (0,)), ((), ())),
                preferred_element_type=jnp.float32,
            )
            block_states_ref[group, at] = added
            block_logs_ref[group, at] = jnp.concatenate(
                [spread(final, way * heads + group * ratio, ratio) for way in range(2)], axis=1
            )
        return 0

    lax.fori_loop(0, count, block, 0)
    logs_total[...] = jnp.zeros_like(logs_total)
    for group in range(groups):

        def onward(at, state):
            return state * jnp.exp(block_logs_ref[group, at][:, :span]) + block_states_ref[
                group, at
            ][:, :span]

        def back(at, state):
            at = count - 1 - at
            return state * jnp.exp(block_logs_ref[group, at][:, span:]) + block_states_ref[
                group, at
            ][:, span:]

        def total(at, carried):
            return carried + block_logs_ref[group, at]

        empty = jnp.zeros((STATE, span), jnp.float32)
        here = slice(group * STATE, (group + 1) * STATE)
        sent_ref[0, here, :] = lax.fori_loop(0, count, onward, empty).astype(jnp.bfloat16)
        sent_ref[1, here, :] = lax.fori_loop(0, count, back, empty).astype(jnp.bfloat16)
        decayed = lax.fori_loop(0, count, total, jnp.zeros((1, 2 * span), jnp.float32))
        coarse = decayed.astype(jnp.bfloat16).astype(jnp.float32)
        logs_total[2 * group : 2 * group + 1, :] = coarse
        logs_total[2 * group + 1 : 2 * group + 2, :] = decayed - coarse
    for way in range(2):
        sent_ref[way, groups * STATE :, :] = logs_total[:, way * span : (way + 1) * span].astype(
            jnp.bfloat16
        )


def diagonal_kernel(shape, signal_ref, inward_ref, outward_ref, within_ref, rows_ref, result_ref):
    groups, ratio, heads = shape
    count = signal_ref.shape[0] // BLOCK
    row = lax.broadcasted_iota(jnp.int32, (BLOCK, BLOCK), 0)
    column = lax.broadcasted_iota(jnp.int32, (BLOCK, BLOCK), 1)
    lane = lax.broadcasted_iota(jnp.int32, (BLOCK, LANES), 1)

    def block(at, _):
        here = pl.ds(pl.multiple_of(at * BLOCK, BLOCK), BLOCK)
        within = within_ref[here, :]
        for group in range(groups):
            intersect = lax.dot_general(
                outward_ref[here, group * STATE : (group + 1) * STATE],
                inward_ref[here, group * STATE : (group + 1) * STATE],
                (((1,), (1,)), ((), ())),
                preferred_element_type=jnp.float32,
            )
            products = []
            for head in range(group * ratio, (group + 1) * ratio):
                other = heads + head
                gap_ahead = within[:, head : head + 1] - rows_ref[head : head + 1, here]
                gap_behind = within[:, other : other + 1] - rows_ref[other : other + 1, here]
                step_ahead = rows_ref[2 * heads + head : 2 * heads + head + 1, here]
                step_behind = rows_ref[2 * heads + other : 2 * heads + other + 1, here]
                gap = jnp.where(row >= column, gap_ahead, gap_behind)
                step = jnp.where(
                    row > column,
                    step_ahead,
                    jnp.where(row < column, step_behind, step_ahead + step_behind),
                )
                weights = (intersect * jnp.exp(gap) * step).astype(jnp.bfloat16)
                tile = head // 2 * 2 * HEAD_DIM
                products.append(
                    jnp.dot(
                        weights,
                        signal_ref[here, tile : tile + LANES],
                        preferred_element_type=jnp.float32,
                    )
                )
            for pair in range(ratio // 2):
                at_tile = (group * ratio + 2 * pair) * HEAD_DIM
                result_ref[here, at_tile : at_tile + LANES] = jnp.where(
                    lane < HEAD_DIM, products[2 * pair], products[2 * pair + 1]
                )
        return 0

    lax.fori_loop(0, count, block, 0)


def finish_kernel(
    shape,
    gathered_ref,
    block_states_ref,
    block_logs_ref,
    outward_ref,
    within_ref,
    diagonal_ref,
    proj_ref,
    gain_ref,
    mixed_ref,
    total,
):
    groups, ratio, heads = shape
    stretches = gathered_ref.shape[0]
    count = outward_ref.shape[0] // BLOCK
    span = ratio * HEAD_DIM
    me = lax.axis_index("sp")
    for group in range(groups):
        states = slice(group * STATE, (group + 1) * STATE)
        log_at = groups * STATE

        def incoming(source, state):
            logs = gathered_ref[source, log_at : log_at + 16, :].astype(jnp.float32)
            logs = logs[2 * group : 2 * group + 1] + logs[2 * group + 1 : 2 * group + 2]
            return state * jnp.exp(logs) + gathered_ref[source, states, :].astype(jnp.float32)

        empty = jnp.zeros((STATE, span), jnp.float32)
        ahead = lax.fori_loop(0, me, incoming, empty)
        behind = lax.fori_loop(
            0,
            stretches - 1 - me,
            lambda hop, state: incoming(stretches - 1 - hop, state),
            empty,
        )
        wide = slice(group * span, (group + 1) * span)

        def back(hop, state):
            at = count - 1 - hop
            here = pl.ds(pl.multiple_of(at * BLOCK, BLOCK), BLOCK)
            carried = jnp.dot(
                outward_ref[here, states],
                state.astype(jnp.bfloat16),
                preferred_element_type=jnp.float32,
            )
            decay = spread(jnp.exp(within_ref[here, :]), heads + group * ratio, ratio)
            total[here, wide] = diagonal_ref[here, wide] + carried * decay
            return (
                state * jnp.exp(block_logs_ref[group, at][:, span:])
                + block_states_ref[group, at][:, span:]
            )

        lax.fori_loop(0, count, back, behind)

        def onward(at, state):
            here = pl.ds(pl.multiple_of(at * BLOCK, BLOCK), BLOCK)
            carried = jnp.dot(
                outward_ref[here, states],
                state.astype(jnp.bfloat16),
                preferred_element_type=jnp.float32,
            )
            decay = spread(jnp.exp(within_ref[here, :]), group * ratio, ratio)
            gate = proj_ref[here, wide].astype(jnp.float32)
            gated = (total[here, wide] + carried * decay) * (gate * sigmoid(gate))
            scale = lax.rsqrt(jnp.mean(gated * gated, axis=-1, keepdims=True) + EPSILON)
            mixed_ref[here, wide] = (gated * scale * gain_ref[:, wide]).astype(jnp.bfloat16)
            return (
                state * jnp.exp(block_logs_ref[group, at][:, :span])
                + block_states_ref[group, at][:, :span]
            )

        lax.fori_loop(0, count, onward, ahead)


def ring_place(index, count):
    outer, inner = index // 2, index % 2
    return (1 - inner) * outer + inner * (count - 1 - outer)


def ring_index(place, count):
    far = place // (count // 2)
    return (1 - far) * (2 * place) + far * (2 * (count - 1 - place) + 1)


def greet(peers):
    barrier = pltpu.get_barrier_semaphore()
    for peer in peers:
        pl.semaphore_signal(
            barrier, inc=1, device_id=peer, device_id_type=pl.DeviceIdType.MESH
        )
    pl.semaphore_wait(barrier, len(peers))


def remote(source, target, send, receive, peer):
    return pltpu.make_async_remote_copy(
        src_ref=source,
        dst_ref=target,
        send_sem=send,
        recv_sem=receive,
        device_id=peer,
        device_id_type=pl.DeviceIdType.MESH,
    )


def gather_kernel(
    stretches,
    parts,
    tokens_ref,
    weights_ref,
    proj_ref,
    edges_ref,
    all_tokens_ref,
    all_weights_ref,
    sums,
    edge_out,
    edge_send,
    edge_receive,
    token_send,
    token_receive,
    ring_send,
    ring_receive,
    own,
):
    me, part = lax.axis_index("sp"), lax.axis_index("tp")
    place = ring_place(me, stretches)
    half_rows = weights_ref.shape[0] // 2
    right = (ring_index((place + 1) % stretches, stretches), part)
    left = (ring_index((place + stretches - 1) % stretches, stretches), part)
    across = [(me, (part + hop) % parts) for hop in range(1, parts)]
    after = ((me + 1) % stretches, part)
    before = ((me + stretches - 1) % stretches, part)
    greet([right, left, after, before] + across)
    rows, depth = tokens_ref.shape[0], weights_ref.shape[0]
    columns = weights_ref.shape[1]

    def project(sources, fresh, final):
        def one(at, _):
            here = pl.ds(pl.multiple_of(at * rows, rows), rows)
            for first in range(0, columns, 2 * LANES):
                tile = slice(first, min(first + 2 * LANES, columns))
                total = None
                for source in sources:
                    if isinstance(source, int):
                        taken = slice(source * depth, (source + 1) * depth)
                    else:
                        taken = pl.ds(pl.multiple_of(source * depth, LANES), depth)
                    term = jnp.dot(
                        all_tokens_ref[at, :, taken],
                        all_weights_ref[source, :, tile],
                        preferred_element_type=jnp.float32,
                    )
                    total = term if total is None else total + term
                if not fresh:
                    total = total + sums[here, tile]
                if final:
                    proj_ref[here, tile] = total.astype(proj_ref.dtype)
                else:
                    sums[here, tile] = total
            return 0

        lax.fori_loop(0, parts, one, 0)

    sends = []
    for hop, peer in enumerate(across):
        copy = remote(
            tokens_ref, all_tokens_ref.at[part], token_send.at[hop], token_receive.at[hop], peer
        )
        copy.start()
        sends.append(copy)
    kept = [
        pltpu.make_async_copy(tokens_ref, all_tokens_ref.at[part], own.at[0]),
        pltpu.make_async_copy(weights_ref, all_weights_ref.at[me], own.at[1]),
    ]
    ring_sends = []
    for hop in range(stretches // 2):
        arriving = []
        for way, peer in enumerate((right, left)):
            source = ring_index((place + stretches + (2 * way - 1) * hop) % stretches, stretches)
            taken = weights_ref if hop == 0 else all_weights_ref.at[source]
            landed = all_weights_ref.at[source]
            if hop == stretches // 2 - 1:
                piece = pl.ds(way * half_rows, half_rows)
                taken, landed = taken.at[piece], landed.at[piece]
            copy = remote(
                taken, landed, ring_send.at[way, hop], ring_receive.at[way, hop], peer
            )
            copy.start()
            arriving.append(copy)
        if hop == 0:
            for copy in kept:
                copy.start()
        if hop == stretches // 2 - 1:
            for copy in sends:
                copy.wait()
            for copy in kept:
                copy.wait()
            if depth % LANES == 0:
                near = [
                    ring_index((place + stretches + away) % stretches, stretches)
                    for away in range(-hop, hop + 1)
                ]
                near[hop] = me
                project(near, True, False)
        for copy in arriving:
            copy.wait_recv()
        ring_sends += arriving
    if depth % LANES == 0:
        opposite = ring_index((place + stretches // 2) % stretches, stretches)
        project([opposite], False, True)
    else:
        project(list(range(stretches)), True, True)
    extent = parts * rows
    edge_out[0] = proj_ref[pl.ds(extent - 16, 16), :]
    edge_out[1] = proj_ref[pl.ds(0, 16), :]
    for copy in ring_sends:
        copy.wait_send()
    edges = [
        remote(edge_out.at[way], edges_ref.at[way], edge_send.at[way], edge_receive.at[way], peer)
        for way, peer in enumerate((after, before))
    ]
    for copy in edges:
        copy.start()
    for copy in edges:
        copy.wait()


def exchange_kernel(
    stretches,
    shape,
    sent_ref,
    signal_ref,
    inward_ref,
    outward_ref,
    within_ref,
    rows_ref,
    gathered_ref,
    result_ref,
    send,
    receive,
):
    me, part = lax.axis_index("sp"), lax.axis_index("tp")
    peers = [(me + hop) % stretches for hop in range(1, stretches)]
    greet([(peer, part) for peer in peers])
    copies = []
    for hop, peer in enumerate(peers):
        wrapped = (me + hop + 1) // stretches
        copy = remote(
            sent_ref.at[wrapped],
            gathered_ref.at[me],
            send.at[hop],
            receive.at[hop],
            (peer, part),
        )
        copy.start()
        copies.append(copy)
    diagonal_kernel(
        shape, signal_ref, inward_ref, outward_ref, within_ref, rows_ref, result_ref
    )
    for copy in copies:
        copy.wait()


def output_kernel(
    mixed_ref,
    weights_ref,
    result_ref,
    near_out,
    near_in,
    far_out,
    far_in,
    own,
    near_send,
    near_receive,
    far_send,
    far_receive,
):
    me, part = lax.axis_index("sp"), lax.axis_index("tp")
    pair, place = part // 2, part % 2
    near = (me, 2 * pair + 1 - place)
    far = (me, 2 * (1 - pair) + place)
    greet([near, far])
    extent = result_ref.shape[0]
    piece = extent // 2
    width = 4 * LANES

    def product(block, at, store):
        start = pl.multiple_of(block * extent + at * piece, piece)
        rows = mixed_ref[pl.ds(start, piece), :]

        def tile(step, _):
            columns = pl.ds(pl.multiple_of(step * width, width), width)
            total = jnp.dot(rows, weights_ref[:, columns], preferred_element_type=jnp.float32)
            store(columns, total)
            return 0

        lax.fori_loop(0, result_ref.shape[1] // width, tile, 0)

    def rows_of(at):
        return pl.ds(at * piece, piece)

    def to_near(block, turn, at):
        def store(columns, total):
            near_out[turn, rows_of(at), columns] = total.astype(jnp.bfloat16)

        product(block, at, store)
        return remote(
            near_out.at[turn, rows_of(at)],
            near_in.at[turn, rows_of(at)],
            near_send.at[turn, at],
            near_receive.at[turn, at],
            near,
        )

    def to_far(block, at, arriving):
        arriving.wait_recv()

        def store(columns, total):
            total = total + near_in[0, rows_of(at), columns].astype(jnp.float32)
            far_out[rows_of(at), columns] = total.astype(jnp.bfloat16)

        product(block, at, store)
        return remote(
            far_out.at[rows_of(at)],
            far_in.at[rows_of(at)],
            far_send.at[at],
            far_receive.at[at],
            far,
        )

    def keep(at):
        def store(columns, total):
            own[rows_of(at), columns] = total

        product(part, at, store)

    theirs, mine = 2 * (1 - pair) + 1 - place, 2 * (1 - pair) + place
    first = [to_near(theirs, 0, 0), None]
    first[1] = to_near(theirs, 0, 1)
    first[0].start()
    keep(0)
    first[1].start()
    keep(1)
    across = [to_far(mine, 0, first[0]), None]
    across[1] = to_far(mine, 1, first[1])
    across[0].start()
    second = [to_near(2 * pair + 1 - place, 1, 0), None]
    across[1].start()
    second[1] = to_near(2 * pair + 1 - place, 1, 1)
    second[0].start()
    second[0].wait_recv()
    own[rows_of(0), :] += near_in[1, rows_of(0), :].astype(jnp.float32)
    second[1].start()
    second[1].wait_recv()
    own[rows_of(1), :] += near_in[1, rows_of(1), :].astype(jnp.float32)
    for at in range(2):
        across[at].wait_recv()
        total = own[rows_of(at), :] + far_in[rows_of(at), :].astype(jnp.float32)
        result_ref[rows_of(at), :] = total.astype(result_ref.dtype)
    for copy in first + second + across:
        copy.wait_send()


def remote_call(body, out_shape, inputs, scratch, collective_id):
    space = pl.BlockSpec(memory_space=pltpu.VMEM)
    return pl.pallas_call(
        body,
        out_shape=out_shape,
        in_specs=[space] * inputs,
        out_specs=jax.tree.map(lambda _: space, out_shape),
        scratch_shapes=scratch,
        cost_estimate=pl.CostEstimate(
            flops=int(3e10), bytes_accessed=1 << 20, transcendentals=0
        ),
        compiler_params=pltpu.CompilerParams(
            collective_id=collective_id, has_side_effects=True, vmem_limit_bytes=VMEM_LIMIT
        ),
    )


def kernel_call(body, out_shape, scratch, micros):
    return pl.pallas_call(
        body,
        out_shape=out_shape,
        scratch_shapes=scratch,
        cost_estimate=pl.CostEstimate(
            flops=int(micros * 5e8), bytes_accessed=1 << 20, transcendentals=0
        ),
        compiler_params=pltpu.CompilerParams(vmem_limit_bytes=VMEM_LIMIT),
    )


def on_device(
    input_activations,
    norm_gain,
    w_gate,
    w_value,
    w_state_in,
    w_state_out,
    w_step_forward,
    w_step_backward,
    step_offset,
    fading_speed,
    conv_value,
    conv_state_in,
    conv_state_out,
    out_gain,
    w_out,
):
    stretches = lax.axis_size("sp")
    content = w_value.shape[1]
    state_width = w_state_in.shape[1]
    heads = w_step_forward.shape[1]
    groups = state_width // STATE
    ratio = heads // groups
    span = ratio * HEAD_DIM
    channels = content + 2 * state_width
    depth = w_gate.shape[0]
    spare = -2 * heads % LANES

    weights = jnp.concatenate(
        [
            w_gate,
            w_value,
            w_state_in,
            w_state_out,
            w_step_forward,
            w_step_backward,
            jnp.zeros((depth, spare), w_gate.dtype),
        ],
        axis=1,
    )
    normed = (rms_rows(input_activations) * norm_gain).astype(jnp.bfloat16)
    parts = lax.axis_size("tp")
    dma = pltpu.SemaphoreType.DMA
    rows_here, features = normed.shape
    extent = parts * rows_here
    count = extent // BLOCK
    wide = weights.shape[1]
    proj, edges = remote_call(
        functools.partial(gather_kernel, stretches, parts),
        (
            jax.ShapeDtypeStruct((extent, wide), normed.dtype),
            jax.ShapeDtypeStruct((2, 16, wide), normed.dtype),
        ),
        2,
        [
            pltpu.VMEM((parts, rows_here, features), normed.dtype),
            pltpu.VMEM((stretches, depth, wide), weights.dtype),
            pltpu.VMEM((extent, wide), jnp.float32),
            pltpu.VMEM((2, 16, wide), normed.dtype),
            dma((2,)),
            dma((2,)),
            dma((parts - 1,)),
            dma((parts - 1,)),
            dma((2, stretches // 2)),
            dma((2, stretches // 2)),
            dma((2,)),
        ],
        1,
    )(normed, weights)
    proj, w_out = lax.optimization_barrier((proj, w_out))
    full_out = lax.all_gather(w_out, "sp", axis=1, tiled=True)

    taps = jnp.concatenate([conv_value, conv_state_in, conv_state_out], axis=1)
    padding = ((0, 0), (0, spare))
    offset = jnp.pad(step_offset.reshape(1, 2 * heads), padding)
    rate = jnp.pad(fading_speed.reshape(1, 2 * heads), padding)
    shift = math.log(extent * stretches)

    bf16, f32 = jnp.bfloat16, jnp.float32
    made = jax.ShapeDtypeStruct
    sent_rows = groups * STATE + 16
    signal, inward, outward, within, rows, block_states, block_logs, sent = kernel_call(
        functools.partial(states_kernel, (groups, ratio, content, state_width, heads, shift)),
        (
            made((extent, content), bf16),
            made((extent, state_width), bf16),
            made((extent, state_width), bf16),
            made((extent, LANES), f32),
            made((4 * heads, extent), f32),
            made((groups, count, STATE, 2 * span), f32),
            made((groups, count, 1, 2 * span), f32),
            made((2, sent_rows, span), bf16),
        ),
        [pltpu.VMEM((extent + 16, channels), f32), pltpu.VMEM((16, 2 * span), f32)],
        15,
    )(proj, edges, taps, offset, rate)
    gathered, diagonal = remote_call(
        functools.partial(exchange_kernel, stretches, (groups, ratio, heads)),
        (made((stretches, sent_rows, span), bf16), made((extent, content), f32)),
        6,
        [dma((stretches - 1,)), dma((stretches - 1,))],
        2,
    )(sent, signal, inward, outward, within, rows)
    mixed = kernel_call(
        functools.partial(finish_kernel, (groups, ratio, heads)),
        made((extent, content), bf16),
        [pltpu.VMEM((extent, content), f32)],
        15,
    )(
        gathered,
        block_states,
        block_logs,
        outward,
        within,
        diagonal,
        proj,
        out_gain.reshape(1, content),
    )
    rows_out, features = input_activations.shape
    if parts != 4:
        partial = jnp.dot(mixed, full_out, preferred_element_type=f32).astype(bf16)
        return lax.psum_scatter(partial, "tp", scatter_dimension=0, tiled=True)
    return remote_call(
        output_kernel,
        made((rows_out, features), bf16),
        2,
        [
            pltpu.VMEM((2, rows_out, features), bf16),
            pltpu.VMEM((2, rows_out, features), bf16),
            pltpu.VMEM((rows_out, features), bf16),
            pltpu.VMEM((rows_out, features), bf16),
            pltpu.VMEM((rows_out, features), f32),
            dma((2, 2)),
            dma((2, 2)),
            dma((2,)),
            dma((2,)),
        ],
        3,
    )(mixed, full_out)


def solution(mesh):
    return jax.shard_map(
        on_device,
        mesh=mesh,
        in_specs=(
            P(("sp", "tp"), None),
            P(),
            P("sp", "tp"),
            P("sp", "tp"),
            P("sp", "tp"),
            P("sp", "tp"),
            P("sp", "tp"),
            P("sp", "tp"),
            P(None, "tp"),
            P(None, "tp"),
            P(None, "tp"),
            P(None, "tp"),
            P(None, "tp"),
            P("tp"),
            P("tp", "sp"),
        ),
        out_specs=P(("sp", "tp"), None),
        check_vma=False,
    )
```

```python
import functools
import math

import jax
import jax.numpy as jnp
from jax import lax
from jax.experimental import pallas as pl
from jax.experimental.pallas import tpu as pltpu
from jax.sharding import PartitionSpec as P

HEAD_DIM = 64
STATE = 128
BLOCK = 128
LANES = 128
EPSILON = 1e-06
HIGHEST = lax.Precision.HIGHEST
VMEM_LIMIT = 60 * 1024 * 1024


def rms_rows(values):
    wide = values.astype(jnp.float32)
    return wide * lax.rsqrt(jnp.mean(wide * wide, axis=-1, keepdims=True) + EPSILON)


def sigmoid(values):
    return 1.0 / (1.0 + jnp.exp(-values))


def softplus(values):
    return jnp.maximum(values, 0.0) + jnp.log1p(jnp.exp(-jnp.abs(values)))


def spread(columns, first, count):
    rows = columns.shape[0]
    lane = lax.broadcasted_iota(jnp.int32, (rows, LANES), 1)
    tiles = []
    for at in range(first, first + count, 2):
        low = jnp.broadcast_to(columns[:, at : at + 1], (rows, LANES))
        high = jnp.broadcast_to(columns[:, at + 1 : at + 2], (rows, LANES))
        tiles.append(jnp.where(lane < HEAD_DIM, low, high))
    return jnp.concatenate(tiles, axis=1)


def states_kernel(
    shape,
    proj_ref,
    edges_ref,
    taps_ref,
    offset_ref,
    rate_ref,
    signal_ref,
    inward_ref,
    outward_ref,
    within_ref,
    rows_ref,
    block_states_ref,
    block_logs_ref,
    sent_ref,
    padded,
    logs_total,
):
    groups, ratio, content, state_width, heads, shift = shape
    extent = proj_ref.shape[0]
    count = extent // BLOCK
    channels = content + 2 * state_width
    span = ratio * HEAD_DIM
    me, last = lax.axis_index("sp"), lax.axis_size("sp") - 1
    low = edges_ref[0, :, content : content + channels].astype(jnp.float32)
    high = edges_ref[1, :, content : content + channels].astype(jnp.float32)
    padded[pl.ds(0, 8), :] = jnp.where(me > 0, low[8:], 0.0)
    padded[pl.ds(extent + 8, 8), :] = jnp.where(me < last, high[:8], 0.0)

    def widen(at, _):
        start = pl.multiple_of(at * BLOCK, BLOCK)
        padded[pl.ds(pl.multiple_of(start + 8, 8), BLOCK), :] = proj_ref[
            pl.ds(start, BLOCK), content : content + channels
        ].astype(jnp.float32)
        return 0

    lax.fori_loop(0, count, widen, 0)
    row = lax.broadcasted_iota(jnp.int32, (BLOCK, BLOCK), 0)
    column = lax.broadcasted_iota(jnp.int32, (BLOCK, BLOCK), 1)
    lower = (row >= column).astype(jnp.float32)
    upper = (row <= column).astype(jnp.float32)
    lane = lax.broadcasted_iota(jnp.int32, (1, LANES), 1)

    def block(at, _):
        start = pl.multiple_of(at * BLOCK, BLOCK)
        here = pl.ds(start, BLOCK)
        filtered = []
        for first in range(0, channels, 2 * LANES):
            part = padded[pl.ds(start, BLOCK + 16), first : first + 2 * LANES]
            taps = taps_ref[:, first : first + 2 * LANES]
            mixed = (
                taps[0:1] * part[7 : 7 + BLOCK]
                + taps[1:2] * part[8 : 8 + BLOCK]
                + taps[2:3] * part[9 : 9 + BLOCK]
            )
            filtered.append((mixed * sigmoid(mixed)).astype(jnp.bfloat16))
        filtered = jnp.concatenate(filtered, axis=1)
        signal = filtered[:, :content]
        inward = filtered[:, content : content + state_width]
        signal_ref[here, :] = signal
        inward_ref[here, :] = inward
        outward_ref[here, :] = filtered[:, content + state_width :]
        raw = proj_ref[here, content + channels :].astype(jnp.float32)
        steps = softplus(raw + offset_ref[...] - shift)
        logs = -steps * rate_ref[...]
        ahead = jnp.dot(lower, logs, precision=HIGHEST, preferred_element_type=jnp.float32)
        behind = jnp.dot(upper, logs, precision=HIGHEST, preferred_element_type=jnp.float32)
        within = jnp.where(lane < heads, ahead, behind)
        final = jnp.where(lane < heads, within[BLOCK - 1 : BLOCK], within[0:1])
        within_ref[here, :] = within
        rows_ref[0 : 2 * heads, here] = within.T[0 : 2 * heads]
        rows_ref[2 * heads : 4 * heads, here] = steps.T[0 : 2 * heads]
        scale = jnp.exp(final - within) * steps
        for group in range(groups):
            wide = signal[:, group * span : (group + 1) * span].astype(jnp.float32)
            scaled = jnp.concatenate(
                [wide * spread(scale, way * heads + group * ratio, ratio) for way in range(2)],
                axis=1,
            ).astype(jnp.bfloat16)
            added = lax.dot_general(
                inward[:, group * STATE : (group + 1) * STATE],
                scaled,
                (((0,), (0,)), ((), ())),
                preferred_element_type=jnp.float32,
            )
            block_states_ref[group, at] = added
            block_logs_ref[group, at] = jnp.concatenate(
                [spread(final, way * heads + group * ratio, ratio) for way in range(2)], axis=1
            )
        return 0

    lax.fori_loop(0, count, block, 0, unroll=2)
    logs_total[...] = jnp.zeros_like(logs_total)
    for group in range(groups):

        def onward(at, state):
            return state * jnp.exp(block_logs_ref[group, at][:, :span]) + block_states_ref[
                group, at
            ][:, :span]

        def back(at, state):
            at = count - 1 - at
            return state * jnp.exp(block_logs_ref[group, at][:, span:]) + block_states_ref[
                group, at
            ][:, span:]

        def total(at, carried):
            return carried + block_logs_ref[group, at]

        empty = jnp.zeros((STATE, span), jnp.float32)
        here = slice(group * STATE, (group + 1) * STATE)
        sent_ref[0, here, :] = lax.fori_loop(0, count, onward, empty).astype(jnp.bfloat16)
        sent_ref[1, here, :] = lax.fori_loop(0, count, back, empty).astype(jnp.bfloat16)
        decayed = lax.fori_loop(0, count, total, jnp.zeros((1, 2 * span), jnp.float32))
        coarse = decayed.astype(jnp.bfloat16).astype(jnp.float32)
        logs_total[2 * group : 2 * group + 1, :] = coarse
        logs_total[2 * group + 1 : 2 * group + 2, :] = decayed - coarse
    for way in range(2):
        sent_ref[way, groups * STATE :, :] = logs_total[:, way * span : (way + 1) * span].astype(
            jnp.bfloat16
        )


def diagonal_kernel(shape, signal_ref, inward_ref, outward_ref, within_ref, rows_ref, result_ref):
    groups, ratio, heads = shape
    count = signal_ref.shape[0] // BLOCK
    row = lax.broadcasted_iota(jnp.int32, (BLOCK, BLOCK), 0)
    column = lax.broadcasted_iota(jnp.int32, (BLOCK, BLOCK), 1)
    lane = lax.broadcasted_iota(jnp.int32, (BLOCK, LANES), 1)

    def block(at, _):
        here = pl.ds(pl.multiple_of(at * BLOCK, BLOCK), BLOCK)
        within = within_ref[here, :]
        for group in range(groups):
            intersect = lax.dot_general(
                outward_ref[here, group * STATE : (group + 1) * STATE],
                inward_ref[here, group * STATE : (group + 1) * STATE],
                (((1,), (1,)), ((), ())),
                preferred_element_type=jnp.float32,
            )
            products = []
            for head in range(group * ratio, (group + 1) * ratio):
                other = heads + head
                gap_ahead = within[:, head : head + 1] - rows_ref[head : head + 1, here]
                gap_behind = within[:, other : other + 1] - rows_ref[other : other + 1, here]
                step_ahead = rows_ref[2 * heads + head : 2 * heads + head + 1, here]
                step_behind = rows_ref[2 * heads + other : 2 * heads + other + 1, here]
                gap = jnp.where(row >= column, gap_ahead, gap_behind)
                step = jnp.where(
                    row > column,
                    step_ahead,
                    jnp.where(row < column, step_behind, step_ahead + step_behind),
                )
                weights = (intersect * jnp.exp(gap) * step).astype(jnp.bfloat16)
                tile = head // 2 * 2 * HEAD_DIM
                products.append(
                    jnp.dot(
                        weights,
                        signal_ref[here, tile : tile + LANES],
                        preferred_element_type=jnp.float32,
                    )
                )
            for pair in range(ratio // 2):
                at_tile = (group * ratio + 2 * pair) * HEAD_DIM
                result_ref[here, at_tile : at_tile + LANES] = jnp.where(
                    lane < HEAD_DIM, products[2 * pair], products[2 * pair + 1]
                )
        return 0

    lax.fori_loop(0, count, block, 0, unroll=2)


def finish_kernel(
    shape,
    gathered_ref,
    block_states_ref,
    block_logs_ref,
    outward_ref,
    within_ref,
    diagonal_ref,
    proj_ref,
    gain_ref,
    mixed_ref,
    total,
):
    groups, ratio, heads = shape
    stretches = gathered_ref.shape[0]
    count = outward_ref.shape[0] // BLOCK
    span = ratio * HEAD_DIM
    me = lax.axis_index("sp")
    for group in range(groups):
        states = slice(group * STATE, (group + 1) * STATE)
        log_at = groups * STATE

        def incoming(source, state):
            logs = gathered_ref[source, log_at : log_at + 16, :].astype(jnp.float32)
            logs = logs[2 * group : 2 * group + 1] + logs[2 * group + 1 : 2 * group + 2]
            return state * jnp.exp(logs) + gathered_ref[source, states, :].astype(jnp.float32)

        empty = jnp.zeros((STATE, span), jnp.float32)
        ahead = lax.fori_loop(0, me, incoming, empty)
        behind = lax.fori_loop(
            0,
            stretches - 1 - me,
            lambda hop, state: incoming(stretches - 1 - hop, state),
            empty,
        )
        wide = slice(group * span, (group + 1) * span)

        def back(hop, state):
            at = count - 1 - hop
            here = pl.ds(pl.multiple_of(at * BLOCK, BLOCK), BLOCK)
            carried = jnp.dot(
                outward_ref[here, states],
                state.astype(jnp.bfloat16),
                preferred_element_type=jnp.float32,
            )
            decay = spread(jnp.exp(within_ref[here, :]), heads + group * ratio, ratio)
            total[here, wide] = diagonal_ref[here, wide] + carried * decay
            return (
                state * jnp.exp(block_logs_ref[group, at][:, span:])
                + block_states_ref[group, at][:, span:]
            )

        lax.fori_loop(0, count, back, behind, unroll=2)

        def onward(at, state):
            here = pl.ds(pl.multiple_of(at * BLOCK, BLOCK), BLOCK)
            carried = jnp.dot(
                outward_ref[here, states],
                state.astype(jnp.bfloat16),
                preferred_element_type=jnp.float32,
            )
            decay = spread(jnp.exp(within_ref[here, :]), group * ratio, ratio)
            gate = proj_ref[here, wide].astype(jnp.float32)
            gated = (total[here, wide] + carried * decay) * (gate * sigmoid(gate))
            scale = lax.rsqrt(jnp.mean(gated * gated, axis=-1, keepdims=True) + EPSILON)
            mixed_ref[here, wide] = (gated * scale * gain_ref[:, wide]).astype(jnp.bfloat16)
            return (
                state * jnp.exp(block_logs_ref[group, at][:, :span])
                + block_states_ref[group, at][:, :span]
            )

        lax.fori_loop(0, count, onward, ahead, unroll=2)


def ring_place(index, count):
    outer, inner = index // 2, index % 2
    return (1 - inner) * outer + inner * (count - 1 - outer)


def ring_index(place, count):
    far = place // (count // 2)
    return (1 - far) * (2 * place) + far * (2 * (count - 1 - place) + 1)


def greet(peers):
    barrier = pltpu.get_barrier_semaphore()
    for peer in peers:
        pl.semaphore_signal(
            barrier, inc=1, device_id=peer, device_id_type=pl.DeviceIdType.MESH
        )
    pl.semaphore_wait(barrier, len(peers))


def remote(source, target, send, receive, peer):
    return pltpu.make_async_remote_copy(
        src_ref=source,
        dst_ref=target,
        send_sem=send,
        recv_sem=receive,
        device_id=peer,
        device_id_type=pl.DeviceIdType.MESH,
    )


def gather_kernel(
    stretches,
    parts,
    tokens_ref,
    weights_ref,
    proj_ref,
    edges_ref,
    all_tokens_ref,
    all_weights_ref,
    sums,
    edge_out,
    edge_send,
    edge_receive,
    token_send,
    token_receive,
    ring_send,
    ring_receive,
    own,
):
    me, part = lax.axis_index("sp"), lax.axis_index("tp")
    place = ring_place(me, stretches)
    half_rows = weights_ref.shape[0] // 2
    right = (ring_index((place + 1) % stretches, stretches), part)
    left = (ring_index((place + stretches - 1) % stretches, stretches), part)
    across = [(me, (part + hop) % parts) for hop in range(1, parts)]
    after = ((me + 1) % stretches, part)
    before = ((me + stretches - 1) % stretches, part)
    greet([right, left, after, before] + across)
    rows, depth = tokens_ref.shape[0], weights_ref.shape[0]
    columns = weights_ref.shape[1]

    def project(sources, fresh, final):
        def one(at, _):
            here = pl.ds(pl.multiple_of(at * rows, rows), rows)
            for first in range(0, columns, 2 * LANES):
                tile = slice(first, min(first + 2 * LANES, columns))
                total = None
                for source in sources:
                    if isinstance(source, int):
                        taken = slice(source * depth, (source + 1) * depth)
                    else:
                        taken = pl.ds(pl.multiple_of(source * depth, LANES), depth)
                    term = jnp.dot(
                        all_tokens_ref[at, :, taken],
                        all_weights_ref[source, :, tile],
                        preferred_element_type=jnp.float32,
                    )
                    total = term if total is None else total + term
                if not fresh:
                    total = total + sums[here, tile]
                if final:
                    proj_ref[here, tile] = total.astype(proj_ref.dtype)
                else:
                    sums[here, tile] = total
            return 0

        lax.fori_loop(0, parts, one, 0)

    sends = []
    for hop, peer in enumerate(across):
        copy = remote(
            tokens_ref, all_tokens_ref.at[part], token_send.at[hop], token_receive.at[hop], peer
        )
        copy.start()
        sends.append(copy)
    kept = [
        pltpu.make_async_copy(tokens_ref, all_tokens_ref.at[part], own.at[0]),
        pltpu.make_async_copy(weights_ref, all_weights_ref.at[me], own.at[1]),
    ]
    ring_sends = []
    for hop in range(stretches // 2):
        arriving = []
        for way, peer in enumerate((right, left)):
            source = ring_index((place + stretches + (2 * way - 1) * hop) % stretches, stretches)
            taken = weights_ref if hop == 0 else all_weights_ref.at[source]
            landed = all_weights_ref.at[source]
            if hop == stretches // 2 - 1:
                piece = pl.ds(way * half_rows, half_rows)
                taken, landed = taken.at[piece], landed.at[piece]
            copy = remote(
                taken, landed, ring_send.at[way, hop], ring_receive.at[way, hop], peer
            )
            copy.start()
            arriving.append(copy)
        if hop == 0:
            for copy in kept:
                copy.start()
        if hop == stretches // 2 - 1:
            for copy in sends:
                copy.wait()
            for copy in kept:
                copy.wait()
            if depth % LANES == 0:
                near = [
                    ring_index((place + stretches + away) % stretches, stretches)
                    for away in range(-hop, hop + 1)
                ]
                near[hop] = me
                project(near, True, False)
        for copy in arriving:
            copy.wait_recv()
        ring_sends += arriving
    if depth % LANES == 0:
        opposite = ring_index((place + stretches // 2) % stretches, stretches)
        project([opposite], False, True)
    else:
        project(list(range(stretches)), True, True)
    extent = parts * rows
    edge_out[0] = proj_ref[pl.ds(extent - 16, 16), :]
    edge_out[1] = proj_ref[pl.ds(0, 16), :]
    for copy in ring_sends:
        copy.wait_send()
    edges = [
        remote(edge_out.at[way], edges_ref.at[way], edge_send.at[way], edge_receive.at[way], peer)
        for way, peer in enumerate((after, before))
    ]
    for copy in edges:
        copy.start()
    for copy in edges:
        copy.wait()


def exchange_kernel(
    stretches,
    shape,
    sent_ref,
    signal_ref,
    inward_ref,
    outward_ref,
    within_ref,
    rows_ref,
    gathered_ref,
    result_ref,
    send,
    receive,
):
    me, part = lax.axis_index("sp"), lax.axis_index("tp")
    peers = [(me + hop) % stretches for hop in range(1, stretches)]
    greet([(peer, part) for peer in peers])
    copies = []
    for hop, peer in enumerate(peers):
        wrapped = (me + hop + 1) // stretches
        copy = remote(
            sent_ref.at[wrapped],
            gathered_ref.at[me],
            send.at[hop],
            receive.at[hop],
            (peer, part),
        )
        copy.start()
        copies.append(copy)
    diagonal_kernel(
        shape, signal_ref, inward_ref, outward_ref, within_ref, rows_ref, result_ref
    )
    for copy in copies:
        copy.wait()


def output_kernel(
    mixed_ref,
    weights_ref,
    result_ref,
    near_out,
    near_in,
    far_out,
    far_in,
    own,
    near_send,
    near_receive,
    far_send,
    far_receive,
):
    me, part = lax.axis_index("sp"), lax.axis_index("tp")
    pair, place = part // 2, part % 2
    near = (me, 2 * pair + 1 - place)
    far = (me, 2 * (1 - pair) + place)
    greet([near, far])
    extent = result_ref.shape[0]
    piece = extent // 2
    width = 4 * LANES

    def product(block, at, store):
        start = pl.multiple_of(block * extent + at * piece, piece)
        rows = mixed_ref[pl.ds(start, piece), :]

        def tile(step, _):
            columns = pl.ds(pl.multiple_of(step * width, width), width)
            total = jnp.dot(rows, weights_ref[:, columns], preferred_element_type=jnp.float32)
            store(columns, total)
            return 0

        lax.fori_loop(0, result_ref.shape[1] // width, tile, 0)

    def rows_of(at):
        return pl.ds(at * piece, piece)

    def to_near(block, turn, at):
        def store(columns, total):
            near_out[turn, rows_of(at), columns] = total.astype(jnp.bfloat16)

        product(block, at, store)
        return remote(
            near_out.at[turn, rows_of(at)],
            near_in.at[turn, rows_of(at)],
            near_send.at[turn, at],
            near_receive.at[turn, at],
            near,
        )

    def to_far(block, at, arriving):
        arriving.wait_recv()

        def store(columns, total):
            total = total + near_in[0, rows_of(at), columns].astype(jnp.float32)
            far_out[rows_of(at), columns] = total.astype(jnp.bfloat16)

        product(block, at, store)
        return remote(
            far_out.at[rows_of(at)],
            far_in.at[rows_of(at)],
            far_send.at[at],
            far_receive.at[at],
            far,
        )

    def keep(at):
        def store(columns, total):
            own[rows_of(at), columns] = total

        product(part, at, store)

    theirs, mine = 2 * (1 - pair) + 1 - place, 2 * (1 - pair) + place
    first = [to_near(theirs, 0, 0), None]
    first[1] = to_near(theirs, 0, 1)
    first[0].start()
    keep(0)
    first[1].start()
    keep(1)
    across = [to_far(mine, 0, first[0]), None]
    across[1] = to_far(mine, 1, first[1])
    across[0].start()
    second = [to_near(2 * pair + 1 - place, 1, 0), None]
    across[1].start()
    second[1] = to_near(2 * pair + 1 - place, 1, 1)
    second[0].start()
    second[0].wait_recv()
    own[rows_of(0), :] += near_in[1, rows_of(0), :].astype(jnp.float32)
    second[1].start()
    second[1].wait_recv()
    own[rows_of(1), :] += near_in[1, rows_of(1), :].astype(jnp.float32)
    for at in range(2):
        across[at].wait_recv()
        total = own[rows_of(at), :] + far_in[rows_of(at), :].astype(jnp.float32)
        result_ref[rows_of(at), :] = total.astype(result_ref.dtype)
    for copy in first + second + across:
        copy.wait_send()


def remote_call(body, out_shape, inputs, scratch, collective_id):
    space = pl.BlockSpec(memory_space=pltpu.VMEM)
    return pl.pallas_call(
        body,
        out_shape=out_shape,
        in_specs=[space] * inputs,
        out_specs=jax.tree.map(lambda _: space, out_shape),
        scratch_shapes=scratch,
        cost_estimate=pl.CostEstimate(
            flops=int(3e10), bytes_accessed=1 << 20, transcendentals=0
        ),
        compiler_params=pltpu.CompilerParams(
            collective_id=collective_id, has_side_effects=True, vmem_limit_bytes=VMEM_LIMIT
        ),
    )


def kernel_call(body, out_shape, scratch, micros):
    return pl.pallas_call(
        body,
        out_shape=out_shape,
        scratch_shapes=scratch,
        cost_estimate=pl.CostEstimate(
            flops=int(micros * 5e8), bytes_accessed=1 << 20, transcendentals=0
        ),
        compiler_params=pltpu.CompilerParams(vmem_limit_bytes=VMEM_LIMIT),
    )


def on_device(
    input_activations,
    norm_gain,
    w_gate,
    w_value,
    w_state_in,
    w_state_out,
    w_step_forward,
    w_step_backward,
    step_offset,
    fading_speed,
    conv_value,
    conv_state_in,
    conv_state_out,
    out_gain,
    w_out,
):
    stretches = lax.axis_size("sp")
    content = w_value.shape[1]
    state_width = w_state_in.shape[1]
    heads = w_step_forward.shape[1]
    groups = state_width // STATE
    ratio = heads // groups
    span = ratio * HEAD_DIM
    channels = content + 2 * state_width
    depth = w_gate.shape[0]
    spare = -2 * heads % LANES

    weights = jnp.concatenate(
        [
            w_gate,
            w_value,
            w_state_in,
            w_state_out,
            w_step_forward,
            w_step_backward,
            jnp.zeros((depth, spare), w_gate.dtype),
        ],
        axis=1,
    )
    full_out = lax.all_gather(w_out, "sp", axis=1, tiled=True)
    normed = (rms_rows(input_activations) * norm_gain).astype(jnp.bfloat16)
    parts = lax.axis_size("tp")
    dma = pltpu.SemaphoreType.DMA
    rows_here, features = normed.shape
    extent = parts * rows_here
    count = extent // BLOCK
    wide = weights.shape[1]
    proj, edges = remote_call(
        functools.partial(gather_kernel, stretches, parts),
        (
            jax.ShapeDtypeStruct((extent, wide), normed.dtype),
            jax.ShapeDtypeStruct((2, 16, wide), normed.dtype),
        ),
        2,
        [
            pltpu.VMEM((parts, rows_here, features), normed.dtype),
            pltpu.VMEM((stretches, depth, wide), weights.dtype),
            pltpu.VMEM((extent, wide), jnp.float32),
            pltpu.VMEM((2, 16, wide), normed.dtype),
            dma((2,)),
            dma((2,)),
            dma((parts - 1,)),
            dma((parts - 1,)),
            dma((2, stretches // 2)),
            dma((2, stretches // 2)),
            dma((2,)),
        ],
        1,
    )(normed, weights)

    taps = jnp.concatenate([conv_value, conv_state_in, conv_state_out], axis=1)
    padding = ((0, 0), (0, spare))
    offset = jnp.pad(step_offset.reshape(1, 2 * heads), padding)
    rate = jnp.pad(fading_speed.reshape(1, 2 * heads), padding)
    shift = math.log(extent * stretches)

    bf16, f32 = jnp.bfloat16, jnp.float32
    made = jax.ShapeDtypeStruct
    sent_rows = groups * STATE + 16
    signal, inward, outward, within, rows, block_states, block_logs, sent = kernel_call(
        functools.partial(states_kernel, (groups, ratio, content, state_width, heads, shift)),
        (
            made((extent, content), bf16),
            made((extent, state_width), bf16),
            made((extent, state_width), bf16),
            made((extent, LANES), f32),
            made((4 * heads, extent), f32),
            made((groups, count, STATE, 2 * span), f32),
            made((groups, count, 1, 2 * span), f32),
            made((2, sent_rows, span), bf16),
        ),
        [pltpu.VMEM((extent + 16, channels), f32), pltpu.VMEM((16, 2 * span), f32)],
        15,
    )(proj, edges, taps, offset, rate)
    gathered, diagonal = remote_call(
        functools.partial(exchange_kernel, stretches, (groups, ratio, heads)),
        (made((stretches, sent_rows, span), bf16), made((extent, content), f32)),
        6,
        [dma((stretches - 1,)), dma((stretches - 1,))],
        2,
    )(sent, signal, inward, outward, within, rows)
    mixed = kernel_call(
        functools.partial(finish_kernel, (groups, ratio, heads)),
        made((extent, content), bf16),
        [pltpu.VMEM((extent, content), f32)],
        15,
    )(
        gathered,
        block_states,
        block_logs,
        outward,
        within,
        diagonal,
        proj,
        out_gain.reshape(1, content),
    )
    rows_out, features = input_activations.shape
    if parts != 4:
        partial = jnp.dot(mixed, full_out, preferred_element_type=f32).astype(bf16)
        return lax.psum_scatter(partial, "tp", scatter_dimension=0, tiled=True)
    return remote_call(
        output_kernel,
        made((rows_out, features), bf16),
        2,
        [
            pltpu.VMEM((2, rows_out, features), bf16),
            pltpu.VMEM((2, rows_out, features), bf16),
            pltpu.VMEM((rows_out, features), bf16),
            pltpu.VMEM((rows_out, features), bf16),
            pltpu.VMEM((rows_out, features), f32),
            dma((2, 2)),
            dma((2, 2)),
            dma((2,)),
            dma((2,)),
        ],
        3,
    )(mixed, full_out)


def solution(mesh):
    return jax.shard_map(
        on_device,
        mesh=mesh,
        in_specs=(
            P(("sp", "tp"), None),
            P(),
            P("sp", "tp"),
            P("sp", "tp"),
            P("sp", "tp"),
            P("sp", "tp"),
            P("sp", "tp"),
            P("sp", "tp"),
            P(None, "tp"),
            P(None, "tp"),
            P(None, "tp"),
            P(None, "tp"),
            P(None, "tp"),
            P("tp"),
            P("tp", "sp"),
        ),
        out_specs=P(("sp", "tp"), None),
        check_vma=False,
    )
```
